32 devices in a mesh: ep: 8 (over z, core), tp: 4 (over y, x).
Axes of the slice: x: 2, y: 2, z: 4, core: 2. Of those that a mesh axis runs over, the one named last changes fastest.
Arguments:
- branch_in: bfloat16 [8192, 512], P(('ep', 'tp')), may hold values from -6 to 6
- pool_weight: bfloat16 [4, 128, 128], replicated, may hold values from -0.5 to 0.5
- group_gain: float32 [512], replicated, may hold values from 0.1 to 1.9
- out_weight: bfloat16 [512, 2048], P(None, 'tp'), may hold values from -0.25 to 0.25
- out_gain: float32 [2048], replicated, may hold values from 0.1 to 1.9
- ffn_input: bfloat16 [1024, 2048], P('ep'), may hold values from -6 to 6
- ffn_gain: float32 [2048], replicated, may hold values from 0.1 to 1.9
- routes: int32 [1024, 4], P('ep'), may hold values from 0 to 7, all different within a row; in each aligned block of 128 rows (0 to 127, 128 to 255, ...) at most 128 rows name the same one
- route_weight: float32 [1024, 4], P('ep'), may hold values from 0.2 to 2
- gate_weight: bfloat16 [8, 2048, 4096], P('ep', None, 'tp'), may hold values from -0.375 to 0.375
- up_weight: bfloat16 [8, 2048, 4096], P('ep', None, 'tp'), may hold values from -0.375 to 0.375
- down_weight: bfloat16 [8, 4096, 2048], P('ep', 'tp'), may hold values from -0.0078125 to 0.0078125
Outputs:
- mixer_out: bfloat16 [8192, 2048], P(('ep', 'tp'))
- expert_out: bfloat16 [1024, 2048], P('ep', 'tp')
The draws below stay inside these ranges and needn't reach their ends.
Inputs may be any that keep to these rules, and one draw needn't show every extreme that they name: `routes`: each row names 4 different experts. Among the 128 rows of one index of ep no expert is named by more than 128 rows, and in some such block one expert is named by exactly 128.
All inputs are finite; a program needn't handle non-finite values.
Results may differ from the reference program's by a relative error of at most 0.017.
Values may be sent and summed in bfloat16 or wider, within the bound.
A program may use at most 64 MiB of HBM per device.

```python
import math
import jax
import jax.numpy as jnp
import numpy as np
from jax import lax

D = 2048
POOL_CH = 128
GW = 512
FF = 4096
TOPK = 4
RA = 256
RB = 128
EXPERTS = 8
CAP = 128
TOKENS_A = 8192
TOKENS_B = 1024
N_EP = 8
N_TP = 4


def block_scale(rng, dims, split, least, largest):
    level = 1.0
    for axis_at, blocks in split:
        draws = jax.random.uniform(jax.random.fold_in(jax.random.fold_in(rng, 6), axis_at), (blocks,), jnp.float32, least / len(split), largest / len(split))
        level = level * jnp.repeat(jnp.exp(draws), dims[axis_at] // blocks).reshape((-1,) + (1,) * (len(dims) - 1 - axis_at))
    return level


def routed_block(stream_key, own, number, rows, amount, top, most, lean):
    ranking = jax.random.permutation(stream_key, amount)
    heavy_load, usual = shares(amount, rows * top, most, lean, True), shares(amount, rows * top, most, lean, False)
    places = jnp.arange(amount)

    def named(lengths, rotation):
        used = int((lengths > 0).sum())
        fixed = max(1, used // 4)
        passed = fixed + (places - fixed + rotation * (used - fixed)) % max(1, amount - fixed)
        return jnp.zeros((amount,), jnp.int32).at[ranking[jnp.where(places < fixed, places, passed)]].set(jnp.asarray(lengths, jnp.int32))

    lengths = jnp.where(number % 4 == 0, named(heavy_load, number // 4), named(usual, number - number // 4 - 1))
    mixed = jax.random.permutation(jax.random.fold_in(own, 3), amount)
    source_of, receiver = mixed[0:amount // 2 * 2:2], mixed[1:amount // 2 * 2:2]
    room = jnp.minimum(lengths[source_of] - 1, most - lengths[receiver]) // 2
    room = jnp.where((source_of == ranking[0]) | (receiver == ranking[0]) | (lengths[receiver] == 0), 0, jnp.maximum(room, 0))
    passed = jax.random.randint(jax.random.fold_in(own, 4), (amount // 2,), 0, 1 << 20) % (room + 1)
    lengths = lengths.at[source_of].add(-passed).at[receiver].add(passed)
    labels = jnp.searchsorted(jnp.cumsum(lengths), jnp.arange(rows * top), side="right").astype(jnp.int32)
    listing = labels.reshape(top, rows).T
    listing = listing[jax.random.permutation(jax.random.fold_in(own, 1), rows)]
    rotation = jax.random.randint(jax.random.fold_in(own, 2), (rows, 1), 0, top)
    return jnp.take_along_axis(listing, (jnp.arange(top)[None, :] + rotation) % top, axis=1)


def shares(number_of, total, limit, skew, full):
    loads = [(1 << 20) // math.isqrt(standing ** skew) + 1 for standing in range(1, number_of + 1)]
    largest = limit if full else min(limit, max(-(-total // number_of), total * loads[0] // sum(loads)))
    least = 1 if total - largest >= number_of - 1 else 0
    holding, rest = [largest] + [least] * (number_of - 1), total - largest - least * (number_of - 1)
    while rest > 0:
        candidates = [i for i in range(1, number_of) if holding[i] < largest] or [i for i in range(1, number_of) if holding[i] < limit]
        pool, remaining = sum([loads[i] for i in candidates]), rest
        for i in candidates:
            addition = min(limit - holding[i], max(1, remaining * loads[i] // pool), rest)
            holding[i] = holding[i] + addition
            rest = rest - addition
    return np.array(holding)


def scatter_about(stream_key, dims, spread, limit, pieces=(), held_as=jnp.bfloat16):
    result = jax.random.normal(stream_key, dims, jnp.float32) * spread
    if len(pieces) > 0:
        result = block_scale(stream_key, dims, pieces, -0.22, 0.18) * result
    return jnp.clip(result, min=-limit, max=limit).astype(held_as)


def setup_inputs(seed: int = 0) -> dict:
    keys = jax.random.split(jax.random.key(seed), 13)
    branch_in = scatter_about(keys[0], (TOKENS_A, GW), 1.0, 6.0, ((0, 32),))
    pool_weight = scatter_about(keys[1], (4, POOL_CH, POOL_CH), POOL_CH ** -0.5, 0.5)
    group_gain = jnp.clip(1.0 + 0.18 * jax.random.normal(keys[2], (GW,), jnp.float32), 0.1, 1.9)
    out_weight = scatter_about(keys[3], (GW, D), GW ** -0.5, 0.25, ((1, 4),))
    out_gain = jnp.clip(1.0 + 0.18 * jax.random.normal(keys[4], (D,), jnp.float32), 0.1, 1.9)
    ffn_input = scatter_about(keys[5], (TOKENS_B, D), 1.0, 6.0, ((0, 8),))
    ffn_gain = jnp.clip(1.0 + 0.18 * jax.random.normal(keys[6], (D,), jnp.float32), 0.1, 1.9)
    routes_keys = jax.random.split(jax.random.fold_in(keys[7], 1), TOKENS_B // RB)
    routes_turns = jax.random.permutation(jax.random.fold_in(keys[7], 3), TOKENS_B // RB)
    routes = jax.vmap(lambda own, number: routed_block(jax.random.fold_in(keys[7], 2), own, number, RB, EXPERTS, TOPK, CAP, 2))(routes_keys, routes_turns).reshape((TOKENS_B, TOPK))
    route_weight = jnp.clip(jnp.exp(math.log(2.0) - 2.3025851 * jax.random.uniform(keys[8], (TOKENS_B, TOPK), jnp.float32) ** block_scale(keys[8], (TOKENS_B, TOPK), ((0, 8),), -0.2, 0.2)), 0.2, 2.0)
    gate_weight = scatter_about(keys[9], (EXPERTS, D, FF), (D // 9) ** -0.5, 0.375, ((0, 8), (2, 4)))
    up_weight = scatter_about(keys[10], (EXPERTS, D, FF), (D // 9) ** -0.5, 0.375, ((0, 8), (2, 4)))
    down_weight = scatter_about(keys[11], (EXPERTS, FF, D), (FF * 160) ** -0.5, 0.0078125, ((0, 8), (1, 4)))
    return dict(branch_in=branch_in, pool_weight=pool_weight, group_gain=group_gain, out_weight=out_weight, out_gain=out_gain, ffn_input=ffn_input, ffn_gain=ffn_gain, routes=routes, route_weight=route_weight, gate_weight=gate_weight, up_weight=up_weight, down_weight=down_weight)


pool_windows = (2, 4, 8, 16)
rim_rows = 15
norm_eps = 1e-06
clamp_limit = 7.0
sigmoid_slope = 1.702

def rms_scale(values, gain):
    return values * lax.rsqrt(lax.optimization_barrier(jnp.mean(values * values, axis=-1, keepdims=True)) + norm_eps) * gain.astype(jnp.float32)

def slot_tables(route_block, expert_count, capacity):
    row_count, top_count = route_block.shape
    flat_experts = route_block.reshape(-1)
    one_hot = (flat_experts[:, None] == jnp.arange(expert_count, dtype=jnp.int32)[None, :]).astype(jnp.int32)
    earlier = jnp.cumsum(one_hot, axis=0) - one_hot
    slot_index = lax.optimization_barrier(jnp.sum(earlier * one_hot, axis=1))
    flat_slots = (slot_index * expert_count + flat_experts).astype(jnp.int32)
    owner_rows = jnp.full((capacity * expert_count,), row_count, jnp.int32)
    owner_rows = owner_rows.at[flat_slots].set(jnp.arange(row_count * top_count, dtype=jnp.int32) // top_count)
    return (flat_slots, owner_rows)

def pool_reference(branch_in, pool_weight, group_gain, out_weight, out_gain):
    total_rows, width = branch_in.shape
    group_chans = width // len(pool_windows)
    widened = jnp.concatenate([jnp.zeros((rim_rows, width), jnp.bfloat16), branch_in], axis=0)
    window = jnp.repeat(jnp.array(pool_windows, jnp.int32), group_chans)

    def one_block(block_index):
        first_row = (block_index * RA).astype(jnp.int32)
        segment = lax.dynamic_slice_in_dim(widened, first_row, RA + rim_rows, 0).astype(jnp.float32)
        positions = first_row + jnp.arange(RA, dtype=jnp.int32)
        summed = jnp.zeros((RA, width), jnp.float32)
        for offset_back in range(rim_rows + 1):
            shifted = segment[rim_rows - offset_back:rim_rows - offset_back + RA]
            summed = summed + jnp.where(window[None, :] > offset_back, shifted, jnp.float32(0.0))
        counts = jnp.minimum(window[None, :], positions[:, None] + 1).astype(jnp.float32)
        pooled = (summed / counts - segment[rim_rows:]).astype(jnp.bfloat16)
        mixed_parts = []
        for group_index in range(len(pool_windows)):
            lower = group_index * group_chans
            mixed_parts.append(jnp.dot(pooled[:, lower:lower + group_chans], pool_weight[group_index], preferred_element_type=jnp.float32))
        group_mix = jnp.concatenate(mixed_parts, axis=1)
        mixed_rows = rms_scale(group_mix, group_gain).astype(jnp.bfloat16)
        projected = jnp.dot(mixed_rows, out_weight, preferred_element_type=jnp.float32)
        return rms_scale(projected, out_gain).astype(jnp.bfloat16)
    blocks = lax.map(one_block, jnp.arange(total_rows // RA, dtype=jnp.int32))
    return blocks.reshape(total_rows, out_weight.shape[1])

def expert_reference(ffn_input, ffn_gain, routes, route_weight, gate_weight, up_weight, down_weight):
    total_rows, model_width = ffn_input.shape
    top_count = routes.shape[1]
    expert_count = gate_weight.shape[0]
    hidden_width = gate_weight.shape[2]
    row_count = total_rows // N_EP
    capacity = 2 * row_count * top_count // expert_count
    normed_rows = rms_scale(ffn_input.astype(jnp.float32), ffn_gain).astype(jnp.bfloat16)
    route_blocks = routes.reshape(N_EP, row_count, top_count)
    flat_slots, owner_rows = jax.vmap(lambda route_block: slot_tables(route_block, expert_count, capacity))(route_blocks)
    padded = jnp.concatenate([normed_rows.reshape(N_EP, row_count, model_width), jnp.zeros((N_EP, 1, model_width), jnp.bfloat16)], axis=1)
    slot_rows = jax.vmap(lambda block_rows, block_owner: block_rows[block_owner])(padded, owner_rows)
    slot_rows = slot_rows.reshape(N_EP, capacity, expert_count, model_width)
    by_expert = jnp.moveaxis(slot_rows, 2, 0).reshape(expert_count, N_EP * capacity, model_width)

    def one_expert(operands):
        expert_rows, gate_local, up_local, down_local = operands
        gate_pre = jnp.minimum(jnp.dot(expert_rows, gate_local, preferred_element_type=jnp.float32), clamp_limit)
        up_pre = jnp.clip(jnp.dot(expert_rows, up_local, preferred_element_type=jnp.float32), -clamp_limit, clamp_limit)
        hidden = ((up_pre + 1.0) * gate_pre * jax.nn.sigmoid(sigmoid_slope * gate_pre)).astype(jnp.bfloat16)
        block_width = hidden_width // N_TP
        part_hidden = hidden.astype(jnp.float32).reshape(expert_rows.shape[0], N_TP, block_width)
        part_down = down_local.astype(jnp.float32).reshape(N_TP, block_width, model_width)
        partials = jnp.einsum('ntf,tfd->tnd', part_hidden, part_down)
        partials = partials.astype(jnp.bfloat16).astype(jnp.float32)
        return lax.optimization_barrier(jnp.sum(partials, axis=0)).astype(jnp.bfloat16)
    results = lax.map(one_expert, (by_expert, gate_weight, up_weight, down_weight))
    results = results.reshape(expert_count, N_EP, capacity, model_width).transpose(1, 2, 0, 3)
    results = results.reshape(N_EP, capacity * expert_count, model_width)
    picked = jax.vmap(lambda block_results, block_slots: block_results[block_slots])(results, flat_slots)
    picked = picked.reshape(total_rows, top_count, model_width).astype(jnp.float32)
    return lax.optimization_barrier(jnp.sum(picked * route_weight[:, :, None], axis=1)).astype(jnp.bfloat16)

def reference(branch_in, pool_weight, group_gain, out_weight, out_gain, ffn_input, ffn_gain, routes, route_weight, gate_weight, up_weight, down_weight):
    mixer_out = pool_reference(branch_in, pool_weight, group_gain, out_weight, out_gain)
    expert_out = expert_reference(ffn_input, ffn_gain, routes, route_weight, gate_weight, up_weight, down_weight)
    return (mixer_out, expert_out)
```

```python
import functools
import math
import jax
import jax.numpy as jnp
from jax import lax
from jax.experimental import pallas as pl
from jax.experimental.pallas import tpu as pltpu
from jax.sharding import PartitionSpec as P

pool_windows = (2, 4, 8, 16)
rim_rows = 16
norm_eps = 1e-06
clamp_limit = 7.0
sigmoid_slope = 1.702
MESH = pl.DeviceIdType.MESH
f32 = jnp.float32
bf16 = jnp.bfloat16


def rms_scale(values, gain):
    return values * lax.rsqrt(jnp.mean(values * values, axis=-1, keepdims=True) + norm_eps) * gain


def grid_of(n_tp):
    nx = 1
    for k in range(1, n_tp + 1):
        if n_tp % k == 0 and k * k <= n_tp:
            nx = k
    return n_tp // nx, nx


def kernel(
    n_ep, n_tp,
    group_gain, out_gain, ffn_gain, routes, route_w, branch_h, pool_h, out_w, x_h, gate_h, up_h, down_h,
    mixer_h, expert_h,
    branch, pool_w, x_own, gate, up, down, xg, wg, rim, ow, hid, mixed, proj, mixer_out, expert_out,
    pown, psend, precv, ts_a, ts_b, t1, u2, t2, fsend, frecv, facc,
    local_sem, sent, r_z, r_x1, r_x2, r_p, r_m, r_t1, r_t2, r_one,
):
    e = lax.axis_index("ep")
    j = lax.axis_index("tp")
    nz = n_ep // 2
    ny, nx = grid_of(n_tp)
    z = e // 2
    c = e % 2
    y = j // nx
    x = j % nx
    rows, width = x_own.shape
    cols = width // n_tp
    half = rows // 2
    qr = rows // 4
    upper = pl.ds(0, half)
    lower = pl.ds(half, half)
    mate = z * 2 + (1 - c)
    last = (j == n_tp - 1).astype(jnp.int32)
    first = (j == 0).astype(jnp.int32)
    nxt = ((e + last) % n_ep, (j + 1) % n_tp)
    prv = ((e - first + n_ep) % n_ep, (j - 1 + n_tp) % n_tp)
    paired = nz & (nz - 1) == 0
    S_Z, S_X1, S_X2, S_P, S_W, S_RIM, S_O, S_O2, S_OP, S_M, S_T1, S_T2, S_F = range(13)
    R_W, R_RIM, R_OA, R_OB, R_O2, R_OP, R_F = range(7)

    def hop(s):
        return (nz - s) % nz

    def partner(s, sign):
        s = hop(s)
        if not paired:
            return (z + sign * s + nz) % nz
        total, bit = 0, 1
        while bit < nz:
            total = total + (z // bit + s // bit) % 2 * bit
            bit *= 2
        return total

    def ep_at(d):
        return partner(d, 1) * 2 + c

    def src_ep(d):
        return partner(d, -1) * 2 + c

    def src_mate(d):
        return partner(d, -1) * 2 + (1 - c)

    def at(dy, dx):
        return (y + dy + ny) % ny * nx + (x + dx + nx) % nx

    def colsl(q):
        return pl.ds(pl.multiple_of(q * cols, cols), cols)

    def send(src, dst, kind, rsem, ep, tp):
        pltpu.make_async_remote_copy(
            src_ref=src, dst_ref=dst, send_sem=sent.at[kind], recv_sem=rsem,
            device_id=(ep, tp), device_id_type=MESH,
        ).start()

    def landed(view, sem):
        pltpu.make_async_copy(view, view, sem).wait()

    steps_x = range(1, nx)
    steps_y = range(1, ny)
    near = nx + ny - 2
    far = (nx - 1) * (ny - 1)

    barrier = pltpu.get_barrier_semaphore()
    for d in range(1, n_ep):
        pl.semaphore_signal(barrier, inc=1, device_id=((e + d) % n_ep, j), device_id_type=MESH)
    for t in range(1, n_tp):
        pl.semaphore_signal(barrier, inc=1, device_id=(e, (j + t) % n_tp), device_id_type=MESH)
    pl.semaphore_signal(barrier, inc=1, device_id=nxt, device_id_type=MESH)
    pl.semaphore_signal(barrier, inc=1, device_id=prv, device_id_type=MESH)

    load_x = pltpu.make_async_copy(x_h, x_own, local_sem.at[0])
    load_branch = pltpu.make_async_copy(branch_h, branch, local_sem.at[1])
    own_ow = pltpu.make_async_copy(out_w, ow.at[j], local_sem.at[2])
    load_pool = pltpu.make_async_copy(pool_h, pool_w, local_sem.at[3])
    loads = [
        pltpu.make_async_copy(gate_h.at[0], gate, local_sem.at[4]),
        pltpu.make_async_copy(up_h.at[0], up, local_sem.at[5]),
        pltpu.make_async_copy(down_h.at[0], down, local_sem.at[6]),
    ]
    write_mixer = pltpu.make_async_copy(mixer_out, mixer_h, local_sem.at[7])
    write_expert = pltpu.make_async_copy(expert_out, expert_h, local_sem.at[8])
    for load in [load_x, load_branch, own_ow, load_pool] + loads:
        load.start()

    chunk = 16

    def norm_rows(i, _):
        r = pl.ds(pl.multiple_of(i * chunk, chunk), chunk)
        xg[e, r, :] = rms_scale(x_own[r, :].astype(f32), ffn_gain[...]).astype(bf16)
        return 0

    experts = lax.broadcasted_iota(jnp.int32, (n_ep, rows), 0)
    named = jnp.zeros((n_ep, rows), f32)
    for k in range(routes.shape[0]):
        named = named + jnp.where(routes[pl.ds(k, 1), :] == experts, route_w[pl.ds(k, 1), :], 0.0)
    wg[e] = named

    def norm_part():
        load_x.wait()
        lax.fori_loop(0, rows // chunk, norm_rows, 0)

    def barrier_wait():
        pl.semaphore_wait(barrier, n_ep - 1 + n_tp - 1 + 2)

    norm_part()
    barrier_wait()

    quart = out_w.shape[0] // 4
    ow_rows = [pl.ds(pl.multiple_of((c * 2 + k) * quart, quart), quart) for k in range(2)]
    my_half = pl.ds(pl.multiple_of(c * 2 * quart, quart), 2 * quart)

    def ow_own(k):
        mine = ow.at[j, ow_rows[k]]
        for dx in steps_x:
            send(mine, mine, S_O, r_one.at[R_OA + k], e, at(0, dx))
        mine = ow.at[j, ow_rows[1 - k]]
        for dy in steps_y:
            send(mine, mine, S_O, r_one.at[R_OA + k], e, at(dy, 0))

    def ow_relay():
        landed(ow.at[pl.ds(0, near), pl.ds(0, quart)], r_one.at[R_OA])
        for dx in steps_x:
            view = ow.at[at(0, -dx), ow_rows[0]]
            for dy in steps_y:
                send(view, view, S_O2, r_one.at[R_O2], e, at(dy, 0))
        for dy in steps_y:
            view = ow.at[at(-dy, 0), ow_rows[1]]
            for dx in steps_x:
                send(view, view, S_O2, r_one.at[R_O2], e, at(0, dx))

    def ow_to_mate():
        landed(ow.at[pl.ds(0, near), pl.ds(0, quart)], r_one.at[R_OB])
        landed(ow.at[pl.ds(0, far), pl.ds(0, 2 * quart)], r_one.at[R_O2])
        for t in range(1, n_tp):
            view = ow.at[(j + t) % n_tp, my_half]
            send(view, view, S_OP, r_one.at[R_OP], mate, j)

    def to_mate(d):
        if not (isinstance(d, int) and d == 0):
            landed(xg.at[0, :, pl.ds(0, far * cols)], r_x2.at[d])
        view = xg.at[src_ep(d)]
        send(view, view, S_P, r_p.at[d], mate, j)

    def start_sends():
        load_branch.wait()
        tail = branch.at[pl.ds(branch.shape[0] - rim_rows, rim_rows)]
        send(tail, rim, S_RIM, r_one.at[R_RIM], nxt[0], nxt[1])
        for d in range(1, n_ep):
            send(wg.at[e], wg.at[e], S_W, r_one.at[R_W], (e + d) % n_ep, j)
        for d in [1, nz - 1] + list(range(2, nz - 1)):
            view = xg.at[e, :, colsl(j)]
            send(view, view, S_Z, r_z.at[d], ep_at(d), j)
        to_mate(0)
        own_ow.wait()
        ow_own(0)
        ow_own(1)

    start_sends()

    branch_rows = branch.shape[0]

    def pool():
        load_pool.wait()
        landed(rim, r_one.at[R_RIM])
        chans = branch.shape[1] // len(pool_windows)
        first_row = (e * n_tp + j) * branch_rows
        positions = first_row + lax.broadcasted_iota(jnp.int32, (branch_rows, 1), 0)
        total = jnp.zeros((branch_rows, 1), f32)
        for g, window in enumerate(pool_windows):
            lanes = slice(g * chans, (g + 1) * chans)
            here = branch[:, lanes].astype(f32)
            edge = jnp.where(first_row == 0, 0.0, rim[:, lanes].astype(f32))
            wide = jnp.concatenate([edge, here], axis=0)
            reach = 1
            while reach < window:
                wide = wide + pltpu.roll(wide, reach, 0)
                reach *= 2
            counts = jnp.minimum(window, positions + 1).astype(f32)
            pooled = (wide[rim_rows:] / counts - here).astype(bf16)
            part = jnp.dot(pooled, pool_w[g], preferred_element_type=f32)
            proj[:, lanes] = part
            total = total + jnp.sum(part * part, axis=-1, keepdims=True)
        scale = lax.rsqrt(total / branch.shape[1] + norm_eps)
        mixed[...] = (proj[:, : branch.shape[1]] * scale * group_gain[...]).astype(bf16)

    def gather_one(d):
        view = xg.at[src_ep(d), :, colsl(j)]
        landed(view, r_z.at[d])
        for dx in steps_x:
            send(view, view, S_X1, r_x1.at[d], e, at(0, dx))
        for dy in steps_y:
            send(view, view, S_X1, r_x1.at[d], e, at(dy, 0))

    def gather_two(d):
        landed(xg.at[0, :, pl.ds(0, near * cols)], r_x1.at[d])
        for dx in steps_x:
            view = xg.at[src_ep(d), upper, colsl(at(0, -dx))]
            for dy in steps_y:
                send(view, view, S_X2, r_x2.at[d], e, at(dy, 0))
        for dy in steps_y:
            view = xg.at[src_ep(d), lower, colsl(at(-dy, 0))]
            for dx in steps_x:
                send(view, view, S_X2, r_x2.at[d], e, at(0, dx))

    diagonal = lax.broadcasted_iota(jnp.int32, (rows, rows), 0) == lax.broadcasted_iota(
        jnp.int32, (rows, rows), 1
    )

    def row_weights(block):
        line = wg[block, pl.ds(e, 1), :]
        return jnp.sum(jnp.where(diagonal, line, 0.0), axis=1, keepdims=True)

    step_f = min(512, gate.shape[1])
    parts_f = gate.shape[1] // step_f

    def hidden_part(s, n):
        span = pl.ds(n * step_f, step_f)
        both = jnp.concatenate([xg[src_ep(s)], xg[src_mate(s)]], axis=0)
        g = jnp.dot(both, gate[:, span], preferred_element_type=f32)
        u = jnp.dot(both, up[:, span], preferred_element_type=f32)
        g = jnp.minimum(g, clamp_limit)
        u = jnp.clip(u, -clamp_limit, clamp_limit)
        hid[:, span] = ((u + 1.0) * g * jax.nn.sigmoid(sigmoid_slope * g)).astype(bf16)

    step_d = min(1024, width)

    def down_part(s):
        mine = row_weights(src_ep(s))
        theirs = row_weights(src_mate(s))

        def one(q, _):
            span = pl.ds(pl.multiple_of(q * step_d, step_d), step_d)
            out = jnp.dot(hid[...], down[:, span], preferred_element_type=f32)
            psend[s, :, span] = (out[rows:] * theirs).astype(bf16)
            pown[s % 2, :, span] = out[:rows] * mine
            send(psend.at[s, :, span], precv.at[s, :, span], S_M, r_m.at[s], mate, j)
            return 0

        lax.fori_loop(0, width // step_d, one, 0)

    def scatter_one(s, h):
        if h == 0:
            landed(precv.at[s], r_m.at[s])
        top = pl.ds(2 * h * qr, qr)
        low = pl.ds((2 * h + 1) * qr, qr)

        def one(q, _):
            a = pown[s % 2, top, colsl(q)] + precv[s, top, colsl(q)].astype(f32)
            b = pown[s % 2, low, colsl(q)] + precv[s, low, colsl(q)].astype(f32)
            ts_a[s, h, q % nx, q // nx] = a.astype(bf16)
            ts_b[s, h, q // nx, q % nx] = b.astype(bf16)
            return 0

        lax.fori_loop(0, n_tp, one, 0)
        for dx in steps_x:
            dst = t1.at[s, h, pl.ds((dx - 1) * ny, ny)]
            send(ts_a.at[s, h, (x + dx) % nx], dst, S_T1, r_t1.at[s, h], e, at(0, dx))
        for dy in steps_y:
            dst = t1.at[s, h, pl.ds((nx - 1) * ny + (dy - 1) * nx, nx)]
            send(ts_b.at[s, h, (y + dy) % ny], dst, S_T1, r_t1.at[s, h], e, at(dy, 0))

    def scatter_two(s, h):
        landed(t1.at[s, h], r_t1.at[s, h])
        for k in range(ny):
            acc = ts_a[s, h, x, k].astype(f32)
            for dx in steps_x:
                acc = acc + t1[s, h, (dx - 1) * ny + k].astype(f32)
            u2[s, h, k] = acc.astype(bf16)
        for k in range(nx):
            acc = ts_b[s, h, y, k].astype(f32)
            for dy in steps_y:
                acc = acc + t1[s, h, (nx - 1) * ny + (dy - 1) * nx + k].astype(f32)
            u2[s, h, ny + k] = acc.astype(bf16)
        for dy in steps_y:
            send(u2.at[s, h, (y + dy) % ny], t2.at[s, h, dy - 1], S_T2, r_t2.at[s, h], e, at(dy, 0))
        for dx in steps_x:
            dst = t2.at[s, h, ny - 1 + dx - 1]
            send(u2.at[s, h, ny + (x + dx) % nx], dst, S_T2, r_t2.at[s, h], e, at(0, dx))

    def scatter_end(s, h):
        landed(t2.at[s, h], r_t2.at[s, h])
        a = u2[s, h, y].astype(f32)
        for dy in steps_y:
            a = a + t2[s, h, dy - 1].astype(f32)
        b = u2[s, h, ny + x].astype(f32)
        for dx in steps_x:
            b = b + t2[s, h, ny - 1 + dx - 1].astype(f32)
        top = pl.ds(2 * h * qr, qr)
        low = pl.ds((2 * h + 1) * qr, qr)
        if isinstance(s, int) and s == 0:
            facc[top] = a
            facc[low] = b
        else:
            fsend[s, top] = a.astype(bf16)
            fsend[s, low] = b.astype(bf16)
            part = pl.ds(2 * h * qr, 2 * qr)
            send(fsend.at[s, part], frecv.at[s, part], S_F, r_one.at[R_F], src_ep(s), j)

    def project():
        landed(ow.at[pl.ds(0, n_tp - 1), pl.ds(0, 2 * quart)], r_one.at[R_OP])

        def one(q, total):
            part = jnp.dot(mixed[...], ow[q], preferred_element_type=f32)
            proj[:, colsl(q)] = part
            return total + jnp.sum(part * part, axis=-1, keepdims=True)

        total = lax.fori_loop(0, n_tp, one, jnp.zeros((branch_rows, 1), f32))
        scale = lax.rsqrt(total / width + norm_eps)

        def two(q, _):
            mixer_out[:, colsl(q)] = (proj[:, colsl(q)] * scale * out_gain[:, colsl(q)]).astype(bf16)
            return 0

        lax.fori_loop(0, n_tp, two, 0)
        write_mixer.start()

    def wait_block(s):
        landed(xg.at[0], r_p.at[s])

    def wait_first():
        for load in loads[:2]:
            load.wait()

    def wait_down():
        loads[2].wait()
        landed(wg.at[pl.ds(0, n_ep - 1)], r_one.at[R_W])

    G1, G2, TM, S1, S2, S3 = gather_one, gather_two, to_mate, scatter_one, scatter_two, scatter_end
    end = nz - 1
    plan = {
        0: (
            [(wait_first,)],
            [],
            [(wait_down,)],
            [(ow_relay,), (pool,), (G1, 1), (G2, 1), (G1, 2), (G1, 3), (TM, 1)],
        ),
        1: ([], [(G2, 2)], [], [(G2, 3), (S1, 1, 0), (S1, 1, 1), (TM, 2)]),
        2: ([], [(TM, 3), (S1, 0, 0)], [(S2, 1, 0), (S1, 0, 1)], [(S2, 1, 1)]),
        end: (
            [],
            [(S1, end - 1, 0), (ow_to_mate,), (S3, end - 2, 0)],
            [(S1, end - 1, 1)],
            [
                (S3, end - 2, 1), (S2, end - 1, 0), (S1, end, 0), (S2, end - 1, 1), (S1, end, 1),
                (S3, end - 1, 0), (project,), (S2, end, 0), (S2, 0, 0), (S3, end - 1, 1), (S2, 0, 1),
                (S2, end, 1), (S3, end, 0), (S3, 0, 0), (S3, end, 1), (S3, 0, 1),
            ],
        ),
    }
    assert nz >= 4

    def middle(s, slot):
        if slot == 1:
            to_mate(s + 1)
            scatter_one(s - 1, 0)
            scatter_end(s - 2, 0)
        if slot == 2:
            scatter_one(s - 1, 1)
        if slot == 3:
            scatter_end(s - 2, 1)
            scatter_two(s - 1, 0)
            scatter_two(s - 1, 1)

    def run(s, slot):
        for i, slots in plan.items():
            if slots[slot]:
                @pl.when(s == i)
                def _():
                    for act in slots[slot]:
                        act[0](*act[1:])

        if nz > 4:
            if slot > 0:
                @pl.when((s > 2) & (s < end))
                def _():
                    middle(s, slot)

            if slot == 3:
                @pl.when((s > 1) & (s + 2 < nz))
                def _():
                    gather_one(s + 2)
                    gather_two(s + 2)

    def step(s, _):
        run(s, 0)
        wait_block(s)
        for n in range(parts_f):
            hidden_part(s, n)
            if n == 0:
                run(s, 1)
        run(s, 2)
        down_part(s)
        run(s, 3)
        return 0

    lax.fori_loop(0, nz, step, 0)

    def drain_all():
        write_mixer.wait()
        landed(fsend.at[pl.ds(1, nz - 1)], sent.at[S_Z])
        landed(xg.at[pl.ds(0, nz - 1), :, pl.ds(0, near * cols)], sent.at[S_X1])
        landed(xg.at[pl.ds(0, nz - 1), :, pl.ds(0, far * cols)], sent.at[S_X2])
        landed(psend, sent.at[S_P])
        landed(wg.at[pl.ds(0, n_ep - 1)], sent.at[S_W])
        landed(rim, sent.at[S_RIM])
        landed(ow.at[pl.ds(0, near), pl.ds(0, 2 * quart)], sent.at[S_O])
        landed(ow.at[pl.ds(0, far), pl.ds(0, 2 * quart)], sent.at[S_O2])
        landed(ow.at[pl.ds(0, n_tp - 1), pl.ds(0, 2 * quart)], sent.at[S_OP])
        landed(psend, sent.at[S_M])
        landed(t1, sent.at[S_T1])
        landed(t2, sent.at[S_T2])

    def final_sum():
        landed(frecv.at[pl.ds(1, nz - 1)], r_one.at[R_F])
        acc = facc[...]
        for d in range(1, nz):
            acc = acc + frecv[d].astype(f32)
        expert_out[...] = acc.astype(bf16)

    def finish():
        write_expert.start()
        landed(fsend.at[pl.ds(1, nz - 1)], sent.at[S_F])
        write_expert.wait()

    drain_all()
    final_sum()
    finish()


def per_device(
    n_ep, n_tp,
    branch_in, pool_weight, group_gain, out_weight, out_gain,
    ffn_input, ffn_gain, routes, route_weight, gate_weight, up_weight, down_weight,
):
    rows, width = ffn_input.shape
    nz = n_ep // 2
    ny, nx = grid_of(n_tp)
    cols = width // n_tp
    qr = rows // 4
    hidden = gate_weight.shape[2]
    branch_rows, branch_width = branch_in.shape
    vm = pl.BlockSpec(memory_space=pltpu.VMEM)
    hbm = pl.BlockSpec(memory_space=pltpu.HBM)
    anyspace = pl.BlockSpec(memory_space=pl.ANY)
    dma = pltpu.SemaphoreType.DMA
    k1 = (nx - 1) * ny + (ny - 1) * nx
    k2 = nx + ny - 2
    buffers = [
        ((branch_rows, branch_width), bf16),
        (pool_weight.shape, bf16),
        ((rows, width), bf16),
        ((width, hidden), bf16),
        ((width, hidden), bf16),
        ((hidden, width), bf16),
        ((n_ep, rows, width), bf16),
        ((n_ep, n_ep, rows), f32),
        ((rim_rows, branch_width), bf16),
        ((n_tp, branch_width, cols), bf16),
        ((2 * rows, hidden), bf16),
        ((branch_rows, branch_width), bf16),
        ((branch_rows, width), f32),
        ((branch_rows, width), bf16),
        ((rows, cols), bf16),
        ((2, rows, width), f32),
        ((nz, rows, width), bf16),
        ((nz, rows, width), bf16),
        ((nz, 2, nx, ny, qr, cols), bf16),
        ((nz, 2, ny, nx, qr, cols), bf16),
        ((nz, 2, k1, qr, cols), bf16),
        ((nz, 2, ny + nx, qr, cols), bf16),
        ((nz, 2, k2, qr, cols), bf16),
        ((nz, rows, cols), bf16),
        ((nz, rows, cols), bf16),
        ((rows, cols), f32),
    ]
    held = sum(math.prod(shape) * jnp.dtype(kind).itemsize for shape, kind in buffers)
    return pl.pallas_call(
        functools.partial(kernel, n_ep, n_tp),
        out_shape=(
            jax.ShapeDtypeStruct((branch_rows, width), bf16),
            jax.ShapeDtypeStruct((rows, cols), bf16),
        ),
        in_specs=[vm] * 5 + [hbm] * 7,
        out_specs=(anyspace, anyspace),
        scratch_shapes=[pltpu.VMEM(shape, kind) for shape, kind in buffers] + [
            dma((9,)), dma((13,)),
            dma((nz,)), dma((nz,)), dma((nz,)), dma((nz,)), dma((nz,)),
            dma((nz, 2)), dma((nz, 2)), dma((7,)),
        ],
        compiler_params=pltpu.CompilerParams(
            collective_id=0, has_side_effects=True, vmem_limit_bytes=67043328
        ),
    )(
        group_gain.reshape(1, -1), out_gain.reshape(1, -1), ffn_gain.reshape(1, -1), routes.T, route_weight.T,
        branch_in, pool_weight, out_weight, ffn_input, gate_weight, up_weight, down_weight,
    )


def solution(mesh):
    in_specs = (
        P(("ep", "tp"), None),
        P(),
        P(),
        P(None, "tp"),
        P(),
        P("ep", None),
        P(),
        P("ep", None),
        P("ep", None),
        P("ep", None, "tp"),
        P("ep", None, "tp"),
        P("ep", "tp", None),
    )
    out_specs = (P(("ep", "tp"), None), P("ep", "tp"))
    return jax.shard_map(
        functools.partial(per_device, mesh.shape["ep"], mesh.shape["tp"]),
        mesh=mesh, in_specs=in_specs, out_specs=out_specs, check_vma=False,
    )
```

```python
import functools
import math
import jax
import jax.numpy as jnp
from jax import lax
from jax.experimental import pallas as pl
from jax.experimental.pallas import tpu as pltpu
from jax.sharding import PartitionSpec as P

pool_windows = (2, 4, 8, 16)
rim_rows = 16
norm_eps = 1e-06
clamp_limit = 7.0
sigmoid_slope = 1.702
MESH = pl.DeviceIdType.MESH
f32 = jnp.float32
bf16 = jnp.bfloat16


def rms_scale(values, gain):
    return values * lax.rsqrt(jnp.mean(values * values, axis=-1, keepdims=True) + norm_eps) * gain


def grid_of(n_tp):
    nx = 1
    for k in range(1, n_tp + 1):
        if n_tp % k == 0 and k * k <= n_tp:
            nx = k
    return n_tp // nx, nx


def kernel(
    n_ep, n_tp,
    group_gain, out_gain, ffn_gain, routes, route_w, branch_h, pool_h, out_w, x_h, gate_h, up_h, down_h,
    mixer_h, expert_h,
    branch, pool_w, x_own, gate, up, down, xg, wg, rim, ow, hid, mixed, proj, mixer_out, expert_out,
    pown, psend, precv, ts_a, ts_b, t1, u2, t2, fsend, frecv, facc,
    local_sem, sent, r_z, r_x1, r_x2, r_p, r_m, r_t1, r_t2, r_one,
):
    e = lax.axis_index("ep")
    j = lax.axis_index("tp")
    nz = n_ep // 2
    ny, nx = grid_of(n_tp)
    z = e // 2
    c = e % 2
    y = j // nx
    x = j % nx
    rows, width = x_own.shape
    cols = width // n_tp
    half = rows // 2
    qr = rows // 4
    upper = pl.ds(0, half)
    lower = pl.ds(half, half)
    mate = z * 2 + (1 - c)
    last = (j == n_tp - 1).astype(jnp.int32)
    first = (j == 0).astype(jnp.int32)
    nxt = ((e + last) % n_ep, (j + 1) % n_tp)
    prv = ((e - first + n_ep) % n_ep, (j - 1 + n_tp) % n_tp)
    paired = nz & (nz - 1) == 0
    S_Z, S_X1, S_X2, S_P, S_W, S_RIM, S_O, S_O2, S_OP, S_M, S_T1, S_T2, S_F = range(13)
    R_W, R_RIM, R_OA, R_OB, R_O2, R_OP, R_F = range(7)

    outer = ((z == 0) | (z == nz - 1)).astype(jnp.int32)

    def hop(s):
        if isinstance(s, int) and s == 0:
            return 0
        turned = s % (nz - 1) + 1
        return s + outer * jnp.where(s == 0, 0, turned - s)

    def partner(m, sign):
        if not paired:
            return (z + sign * m + nz) % nz
        total, bit = 0, 1
        while bit < nz:
            total = total + (z // bit + m // bit) % 2 * bit
            bit *= 2
        return total

    def src_ep(s):
        return partner(hop(s), -1) * 2 + c

    def src_mate(s):
        return partner(hop(s), -1) * 2 + (1 - c)

    def at(dy, dx):
        return (y + dy + ny) % ny * nx + (x + dx + nx) % nx

    def colsl(q):
        return pl.ds(pl.multiple_of(q * cols, cols), cols)

    def send(src, dst, kind, rsem, ep, tp):
        pltpu.make_async_remote_copy(
            src_ref=src, dst_ref=dst, send_sem=sent.at[kind], recv_sem=rsem,
            device_id=(ep, tp), device_id_type=MESH,
        ).start()

    def landed(view, sem):
        pltpu.make_async_copy(view, view, sem).wait()

    steps_x = range(1, nx)
    steps_y = range(1, ny)
    near = nx + ny - 2
    far = (nx - 1) * (ny - 1)

    barrier = pltpu.get_barrier_semaphore()
    for d in range(1, n_ep):
        pl.semaphore_signal(barrier, inc=1, device_id=((e + d) % n_ep, j), device_id_type=MESH)
    for t in range(1, n_tp):
        pl.semaphore_signal(barrier, inc=1, device_id=(e, (j + t) % n_tp), device_id_type=MESH)
    pl.semaphore_signal(barrier, inc=1, device_id=nxt, device_id_type=MESH)
    pl.semaphore_signal(barrier, inc=1, device_id=prv, device_id_type=MESH)

    load_x = pltpu.make_async_copy(x_h, x_own, local_sem.at[0])
    load_branch = pltpu.make_async_copy(branch_h, branch, local_sem.at[1])
    own_ow = pltpu.make_async_copy(out_w, ow.at[j], local_sem.at[2])
    load_pool = pltpu.make_async_copy(pool_h, pool_w, local_sem.at[3])
    loads = [
        pltpu.make_async_copy(gate_h.at[0], gate, local_sem.at[4]),
        pltpu.make_async_copy(up_h.at[0], up, local_sem.at[5]),
        pltpu.make_async_copy(down_h.at[0], down, local_sem.at[6]),
    ]
    write_mixer = pltpu.make_async_copy(mixer_out, mixer_h, local_sem.at[7])
    write_expert = pltpu.make_async_copy(expert_out, expert_h, local_sem.at[8])
    for load in [load_x, load_branch, own_ow, load_pool] + loads:
        load.start()

    chunk = 16

    def norm_rows(i, _):
        r = pl.ds(pl.multiple_of(i * chunk, chunk), chunk)
        xg[e, r, :] = rms_scale(x_own[r, :].astype(f32), ffn_gain[...]).astype(bf16)
        return 0

    experts = lax.broadcasted_iota(jnp.int32, (n_ep, rows), 0)
    named = jnp.zeros((n_ep, rows), f32)
    for k in range(routes.shape[0]):
        named = named + jnp.where(routes[pl.ds(k, 1), :] == experts, route_w[pl.ds(k, 1), :], 0.0)
    wg[e] = named

    def norm_part():
        load_x.wait()
        lax.fori_loop(0, rows // chunk, norm_rows, 0)

    def barrier_wait():
        pl.semaphore_wait(barrier, n_ep - 1 + n_tp - 1 + 2)

    norm_part()
    barrier_wait()

    quart = out_w.shape[0] // 4
    ow_rows = [pl.ds(pl.multiple_of((c * 2 + k) * quart, quart), quart) for k in range(2)]
    my_half = pl.ds(pl.multiple_of(c * 2 * quart, quart), 2 * quart)

    def ow_own(k):
        mine = ow.at[j, ow_rows[k]]
        for dx in steps_x:
            send(mine, mine, S_O, r_one.at[R_OA + k], e, at(0, dx))
        mine = ow.at[j, ow_rows[1 - k]]
        for dy in steps_y:
            send(mine, mine, S_O, r_one.at[R_OA + k], e, at(dy, 0))

    def ow_relay():
        landed(ow.at[pl.ds(0, near), pl.ds(0, quart)], r_one.at[R_OA])
        for dx in steps_x:
            view = ow.at[at(0, -dx), ow_rows[0]]
            for dy in steps_y:
                send(view, view, S_O2, r_one.at[R_O2], e, at(dy, 0))
        for dy in steps_y:
            view = ow.at[at(-dy, 0), ow_rows[1]]
            for dx in steps_x:
                send(view, view, S_O2, r_one.at[R_O2], e, at(0, dx))

    def ow_to_mate():
        landed(ow.at[pl.ds(0, near), pl.ds(0, quart)], r_one.at[R_OB])
        landed(ow.at[pl.ds(0, far), pl.ds(0, 2 * quart)], r_one.at[R_O2])
        for t in range(1, n_tp):
            view = ow.at[(j + t) % n_tp, my_half]
            send(view, view, S_OP, r_one.at[R_OP], mate, j)

    def to_mate(d):
        if not (isinstance(d, int) and d == 0):
            landed(xg.at[0, :, pl.ds(0, far * cols)], r_x2.at[d])
        view = xg.at[src_ep(d)]
        send(view, view, S_P, r_p.at[d], mate, j)

    def send_block(m):
        view = xg.at[e, :, colsl(j)]
        send(view, view, S_Z, r_z.at[m], partner(m, 1) * 2 + c, j)

    def send_rest():
        pl.when(outer == 0)(lambda: send_block(nz - 1))
        ow_own(1)

    def start_sends():
        load_branch.wait()
        tail = branch.at[pl.ds(branch.shape[0] - rim_rows, rim_rows)]
        send(tail, rim, S_RIM, r_one.at[R_RIM], nxt[0], nxt[1])
        for d in range(1, n_ep):
            send(wg.at[e], wg.at[e], S_W, r_one.at[R_W], (e + d) % n_ep, j)
        for m in range(1, nz - 1):
            send_block(m)
        pl.when(outer == 1)(lambda: send_block(nz - 1))
        to_mate(0)
        own_ow.wait()
        ow_own(0)

    start_sends()

    branch_rows = branch.shape[0]

    def pool():
        load_pool.wait()
        landed(rim, r_one.at[R_RIM])
        chans = branch.shape[1] // len(pool_windows)
        first_row = (e * n_tp + j) * branch_rows
        positions = first_row + lax.broadcasted_iota(jnp.int32, (branch_rows, 1), 0)
        total = jnp.zeros((branch_rows, 1), f32)
        for g, window in enumerate(pool_windows):
            lanes = slice(g * chans, (g + 1) * chans)
            here = branch[:, lanes].astype(f32)
            edge = jnp.where(first_row == 0, 0.0, rim[:, lanes].astype(f32))
            wide = jnp.concatenate([edge, here], axis=0)
            reach = 1
            while reach < window:
                wide = wide + pltpu.roll(wide, reach, 0)
                reach *= 2
            counts = jnp.minimum(window, positions + 1).astype(f32)
            pooled = (wide[rim_rows:] / counts - here).astype(bf16)
            part = jnp.dot(pooled, pool_w[g], preferred_element_type=f32)
            proj[:, lanes] = part
            total = total + jnp.sum(part * part, axis=-1, keepdims=True)
        scale = lax.rsqrt(total / branch.shape[1] + norm_eps)
        mixed[...] = (proj[:, : branch.shape[1]] * scale * group_gain[...]).astype(bf16)

    def gather_one(d):
        view = xg.at[src_ep(d), :, colsl(j)]
        landed(view, r_z.at[hop(d)])
        for dx in steps_x:
            send(view, view, S_X1, r_x1.at[d], e, at(0, dx))
        for dy in steps_y:
            send(view, view, S_X1, r_x1.at[d], e, at(dy, 0))

    def gather_two(d):
        landed(xg.at[0, :, pl.ds(0, near * cols)], r_x1.at[d])
        for dx in steps_x:
            view = xg.at[src_ep(d), upper, colsl(at(0, -dx))]
            for dy in steps_y:
                send(view, view, S_X2, r_x2.at[d], e, at(dy, 0))
        for dy in steps_y:
            view = xg.at[src_ep(d), lower, colsl(at(-dy, 0))]
            for dx in steps_x:
                send(view, view, S_X2, r_x2.at[d], e, at(0, dx))

    diagonal = lax.broadcasted_iota(jnp.int32, (rows, rows), 0) == lax.broadcasted_iota(
        jnp.int32, (rows, rows), 1
    )

    def row_weights(block):
        line = wg[block, pl.ds(e, 1), :]
        return jnp.sum(jnp.where(diagonal, line, 0.0), axis=1, keepdims=True)

    step_f = min(512, gate.shape[1])
    parts_f = gate.shape[1] // step_f

    def hidden_part(s, n):
        span = pl.ds(n * step_f, step_f)
        both = jnp.concatenate([xg[src_ep(s)], xg[src_mate(s)]], axis=0)
        g = jnp.dot(both, gate[:, span], preferred_element_type=f32)
        u = jnp.dot(both, up[:, span], preferred_element_type=f32)
        g = jnp.minimum(g, clamp_limit)
        u = jnp.clip(u, -clamp_limit, clamp_limit)
        hid[:, span] = ((u + 1.0) * g * jax.nn.sigmoid(sigmoid_slope * g)).astype(bf16)

    step_d = min(1024, width)

    def down_part(s):
        mine = row_weights(src_ep(s))
        theirs = row_weights(src_mate(s))

        def one(q, _):
            span = pl.ds(pl.multiple_of(q * step_d, step_d), step_d)
            out = jnp.dot(hid[...], down[:, span], preferred_element_type=f32)
            psend[s, :, span] = (out[rows:] * theirs).astype(bf16)
            pown[s % 2, :, span] = out[:rows] * mine
            send(psend.at[s, :, span], precv.at[s, :, span], S_M, r_m.at[s], mate, j)
            return 0

        lax.fori_loop(0, width // step_d, one, 0)

    def scatter_one(s, h):
        if h == 0:
            landed(precv.at[s], r_m.at[s])
        top = pl.ds(2 * h * qr, qr)
        low = pl.ds((2 * h + 1) * qr, qr)

        def one(q, _):
            a = pown[s % 2, top, colsl(q)] + precv[s, top, colsl(q)].astype(f32)
            b = pown[s % 2, low, colsl(q)] + precv[s, low, colsl(q)].astype(f32)
            ts_a[s, h, q % nx, q // nx] = a.astype(bf16)
            ts_b[s, h, q // nx, q % nx] = b.astype(bf16)
            return 0

        lax.fori_loop(0, n_tp, one, 0)
        for dx in steps_x:
            dst = t1.at[s, h, pl.ds((dx - 1) * ny, ny)]
            send(ts_a.at[s, h, (x + dx) % nx], dst, S_T1, r_t1.at[s, h], e, at(0, dx))
        for dy in steps_y:
            dst = t1.at[s, h, pl.ds((nx - 1) * ny + (dy - 1) * nx, nx)]
            send(ts_b.at[s, h, (y + dy) % ny], dst, S_T1, r_t1.at[s, h], e, at(dy, 0))

    def scatter_two(s, h):
        landed(t1.at[s, h], r_t1.at[s, h])
        for k in range(ny):
            acc = ts_a[s, h, x, k].astype(f32)
            for dx in steps_x:
                acc = acc + t1[s, h, (dx - 1) * ny + k].astype(f32)
            u2[s, h, k] = acc.astype(bf16)
        for k in range(nx):
            acc = ts_b[s, h, y, k].astype(f32)
            for dy in steps_y:
                acc = acc + t1[s, h, (nx - 1) * ny + (dy - 1) * nx + k].astype(f32)
            u2[s, h, ny + k] = acc.astype(bf16)
        for dy in steps_y:
            send(u2.at[s, h, (y + dy) % ny], t2.at[s, h, dy - 1], S_T2, r_t2.at[s, h], e, at(dy, 0))
        for dx in steps_x:
            dst = t2.at[s, h, ny - 1 + dx - 1]
            send(u2.at[s, h, ny + (x + dx) % nx], dst, S_T2, r_t2.at[s, h], e, at(0, dx))

    def scatter_end(s, h):
        landed(t2.at[s, h], r_t2.at[s, h])
        a = u2[s, h, y].astype(f32)
        for dy in steps_y:
            a = a + t2[s, h, dy - 1].astype(f32)
        b = u2[s, h, ny + x].astype(f32)
        for dx in steps_x:
            b = b + t2[s, h, ny - 1 + dx - 1].astype(f32)
        top = pl.ds(2 * h * qr, qr)
        low = pl.ds((2 * h + 1) * qr, qr)
        if isinstance(s, int) and s == 0:
            facc[top] = a
            facc[low] = b
        else:
            fsend[s, top] = a.astype(bf16)
            fsend[s, low] = b.astype(bf16)
            part = pl.ds(2 * h * qr, 2 * qr)
            send(fsend.at[s, part], frecv.at[hop(s), part], S_F, r_one.at[R_F], src_ep(s), j)

    def project():
        landed(ow.at[pl.ds(0, n_tp - 1), pl.ds(0, 2 * quart)], r_one.at[R_OP])

        def one(q, total):
            part = jnp.dot(mixed[...], ow[q], preferred_element_type=f32)
            proj[:, colsl(q)] = part
            return total + jnp.sum(part * part, axis=-1, keepdims=True)

        total = lax.fori_loop(0, n_tp, one, jnp.zeros((branch_rows, 1), f32))
        scale = lax.rsqrt(total / width + norm_eps)

        def two(q, _):
            mixer_out[:, colsl(q)] = (proj[:, colsl(q)] * scale * out_gain[:, colsl(q)]).astype(bf16)
            return 0

        lax.fori_loop(0, n_tp, two, 0)
        write_mixer.start()

    def wait_block(s):
        landed(xg.at[0], r_p.at[s])

    def wait_first():
        for load in loads[:2]:
            load.wait()

    def wait_down():
        loads[2].wait()
        landed(wg.at[pl.ds(0, n_ep - 1)], r_one.at[R_W])

    G1, G2, TM, S1, S2, S3 = gather_one, gather_two, to_mate, scatter_one, scatter_two, scatter_end
    end = nz - 1
    plan = {
        0: (
            [(wait_first,)],
            [(send_rest,)],
            [(wait_down,)],
            [(G1, 1), (pool,), (S1, 0, 0), (G2, 1), (G1, 2), (TM, 1), (G1, 3)],
        ),
        1: ([], [(G2, 2)], [(ow_relay,)], [(G2, 3), (S1, 1, 0), (TM, 2)]),
        2: ([], [(S1, 1, 1)], [(S1, 0, 1), (TM, 3)], [(S2, 1, 0), (ow_to_mate,)]),
        end: (
            [],
            [(S1, end - 1, 0)],
            [(S2, end - 2, 1), (S1, end - 1, 1), (S3, end - 2, 0)],
            [
                (S2, end - 1, 0), (S3, end - 2, 1), (S1, end, 0), (S2, end - 1, 1), (S1, end, 1),
                (S3, end - 1, 0), (S2, 0, 0), (project,), (S2, end, 0), (S2, 0, 1), (S3, end - 1, 1),
                (S2, end, 1), (S3, end, 0), (S3, 0, 0), (S3, end, 1), (S3, 0, 1),
            ],
        ),
    }
    assert nz >= 4

    def middle(s, slot):
        if slot == 1:
            scatter_one(s - 1, 0)
        if slot == 2:
            scatter_two(s - 2, 1)
            scatter_one(s - 1, 1)
            scatter_end(s - 2, 0)
            to_mate(s + 1)
        if slot == 3:
            scatter_two(s - 1, 0)
            scatter_end(s - 2, 1)

    def run(s, slot):
        for i, slots in plan.items():
            if slots[slot]:
                @pl.when(s == i)
                def _():
                    for act in slots[slot]:
                        act[0](*act[1:])

        if nz > 4:
            if slot > 0:
                @pl.when((s > 2) & (s < end))
                def _():
                    middle(s, slot)

            if slot == 3:
                @pl.when((s > 1) & (s + 2 < nz))
                def _():
                    gather_one(s + 2)
                    gather_two(s + 2)

    def step(s, _):
        run(s, 0)
        wait_block(s)
        for n in range(parts_f):
            hidden_part(s, n)
            if n == 0:
                run(s, 1)
        run(s, 2)
        down_part(s)
        run(s, 3)
        return 0

    lax.fori_loop(0, nz, step, 0)

    def drain_all():
        write_mixer.wait()
        landed(fsend.at[pl.ds(1, nz - 1)], sent.at[S_Z])
        landed(xg.at[pl.ds(0, nz - 1), :, pl.ds(0, near * cols)], sent.at[S_X1])
        landed(xg.at[pl.ds(0, nz - 1), :, pl.ds(0, far * cols)], sent.at[S_X2])
        landed(psend, sent.at[S_P])
        landed(wg.at[pl.ds(0, n_ep - 1)], sent.at[S_W])
        landed(rim, sent.at[S_RIM])
        landed(ow.at[pl.ds(0, near), pl.ds(0, 2 * quart)], sent.at[S_O])
        landed(ow.at[pl.ds(0, far), pl.ds(0, 2 * quart)], sent.at[S_O2])
        landed(ow.at[pl.ds(0, n_tp - 1), pl.ds(0, 2 * quart)], sent.at[S_OP])
        landed(psend, sent.at[S_M])
        landed(t1, sent.at[S_T1])
        landed(t2, sent.at[S_T2])

    def final_sum():
        landed(frecv.at[pl.ds(1, nz - 1)], r_one.at[R_F])
        acc = facc[...]
        for d in range(1, nz):
            acc = acc + frecv[d].astype(f32)
        expert_out[...] = acc.astype(bf16)

    def finish():
        write_expert.start()
        landed(fsend.at[pl.ds(1, nz - 1)], sent.at[S_F])
        write_expert.wait()

    drain_all()
    final_sum()
    finish()


def per_device(
    n_ep, n_tp,
    branch_in, pool_weight, group_gain, out_weight, out_gain,
    ffn_input, ffn_gain, routes, route_weight, gate_weight, up_weight, down_weight,
):
    rows, width = ffn_input.shape
    nz = n_ep // 2
    ny, nx = grid_of(n_tp)
    cols = width // n_tp
    qr = rows // 4
    hidden = gate_weight.shape[2]
    branch_rows, branch_width = branch_in.shape
    vm = pl.BlockSpec(memory_space=pltpu.VMEM)
    hbm = pl.BlockSpec(memory_space=pltpu.HBM)
    anyspace = pl.BlockSpec(memory_space=pl.ANY)
    dma = pltpu.SemaphoreType.DMA
    k1 = (nx - 1) * ny + (ny - 1) * nx
    k2 = nx + ny - 2
    buffers = [
        ((branch_rows, branch_width), bf16),
        (pool_weight.shape, bf16),
        ((rows, width), bf16),
        ((width, hidden), bf16),
        ((width, hidden), bf16),
        ((hidden, width), bf16),
        ((n_ep, rows, width), bf16),
        ((n_ep, n_ep, rows), f32),
        ((rim_rows, branch_width), bf16),
        ((n_tp, branch_width, cols), bf16),
        ((2 * rows, hidden), bf16),
        ((branch_rows, branch_width), bf16),
        ((branch_rows, width), f32),
        ((branch_rows, width), bf16),
        ((rows, cols), bf16),
        ((2, rows, width), f32),
        ((nz, rows, width), bf16),
        ((nz, rows, width), bf16),
        ((nz, 2, nx, ny, qr, cols), bf16),
        ((nz, 2, ny, nx, qr, cols), bf16),
        ((nz, 2, k1, qr, cols), bf16),
        ((nz, 2, ny + nx, qr, cols), bf16),
        ((nz, 2, k2, qr, cols), bf16),
        ((nz, rows, cols), bf16),
        ((nz, rows, cols), bf16),
        ((rows, cols), f32),
    ]
    operands = (
        group_gain.reshape(1, -1), out_gain.reshape(1, -1), ffn_gain.reshape(1, -1), routes.T, route_weight.T,
        branch_in, pool_weight, out_weight, ffn_input, gate_weight, up_weight, down_weight,
    )
    held = sum(math.prod(shape) * jnp.dtype(kind).itemsize for shape, kind in buffers)
    return pl.pallas_call(
        functools.partial(kernel, n_ep, n_tp),
        out_shape=(
            jax.ShapeDtypeStruct((branch_rows, width), bf16),
            jax.ShapeDtypeStruct((rows, cols), bf16),
        ),
        in_specs=[vm] * 5 + [hbm] * 7,
        out_specs=(anyspace, anyspace),
        scratch_shapes=[pltpu.VMEM(shape, kind) for shape, kind in buffers] + [
            dma((9,)), dma((13,)),
            dma((nz,)), dma((nz,)), dma((nz,)), dma((nz,)), dma((nz,)),
            dma((nz, 2)), dma((nz, 2)), dma((7,)),
        ],
        compiler_params=pltpu.CompilerParams(
            collective_id=0, has_side_effects=True, vmem_limit_bytes=min(67043328, held + (8 << 20))
        ),
    )(
        *[pltpu.with_memory_space_constraint(v, pltpu.HBM) for v in operands]
    )


def solution(mesh):
    in_specs = (
        P(("ep", "tp"), None),
        P(),
        P(),
        P(None, "tp"),
        P(),
        P("ep", None),
        P(),
        P("ep", None),
        P("ep", None),
        P("ep", None, "tp"),
        P("ep", None, "tp"),
        P("ep", "tp", None),
    )
    out_specs = (P(("ep", "tp"), None), P("ep", "tp"))
    return jax.shard_map(
        functools.partial(per_device, mesh.shape["ep"], mesh.shape["tp"]),
        mesh=mesh, in_specs=in_specs, out_specs=out_specs, check_vma=False,
    )
```

```python
import functools
import math
import jax
import jax.numpy as jnp
from jax import lax
from jax.experimental import pallas as pl
from jax.experimental.pallas import tpu as pltpu
from jax.sharding import PartitionSpec as P

pool_windows = (2, 4, 8, 16)
rim_rows = 16
norm_eps = 1e-06
clamp_limit = 7.0
sigmoid_slope = 1.702
MESH = pl.DeviceIdType.MESH
f32 = jnp.float32
bf16 = jnp.bfloat16


def rms_scale(values, gain):
    return values * lax.rsqrt(jnp.mean(values * values, axis=-1, keepdims=True) + norm_eps) * gain


def grid_of(n_tp):
    nx = 1
    for k in range(1, n_tp + 1):
        if n_tp % k == 0 and k * k <= n_tp:
            nx = k
    return n_tp // nx, nx


def kernel(
    n_ep, n_tp,
    group_gain_h, out_gain_h, ffn_gain_h, routes_h, route_w_h, branch_h, pool_h, out_w, x_h,
    gate_h, up_h, down_h,
    mixer_h, expert_h,
    group_gain, out_gain, ffn_gain, routes, route_w, branch, pool_w, x_own, gate, up, down, xg, wg, rim, ow, hid, mixed, proj, mixer_out, expert_out,
    pown, psend, precv, ts_a, ts_b, t1, u2, t2, fsend, frecv, facc,
    local_sem, sent, r_z, r_x1, r_x2, r_p, r_m, r_t1, r_t2, r_one,
):
    e = lax.axis_index("ep")
    j = lax.axis_index("tp")
    nz = n_ep // 2
    ny, nx = grid_of(n_tp)
    z = e // 2
    c = e % 2
    y = j // nx
    x = j % nx
    rows, width = x_own.shape
    cols = width // n_tp
    half = rows // 2
    qr = rows // 4
    upper = pl.ds(0, half)
    lower = pl.ds(half, half)
    mate = z * 2 + (1 - c)
    last = (j == n_tp - 1).astype(jnp.int32)
    first = (j == 0).astype(jnp.int32)
    nxt = ((e + last) % n_ep, (j + 1) % n_tp)
    prv = ((e - first + n_ep) % n_ep, (j - 1 + n_tp) % n_tp)
    paired = nz & (nz - 1) == 0
    S_Z, S_X1, S_X2, S_P, S_W, S_RIM, S_O, S_O2, S_OP, S_M, S_T1, S_T2, S_F = range(13)
    R_W, R_RIM, R_OA, R_OB, R_O2, R_OP, R_F = range(7)

    outer = ((z == 0) | (z == nz - 1)).astype(jnp.int32)

    def hop(s):
        if isinstance(s, int) and s == 0:
            return 0
        turned = s % (nz - 1) + 1
        return s + outer * jnp.where(s == 0, 0, turned - s)

    def partner(m, sign):
        if not paired:
            return (z + sign * m + nz) % nz
        total, bit = 0, 1
        while bit < nz:
            total = total + (z // bit + m // bit) % 2 * bit
            bit *= 2
        return total

    def src_ep(s):
        return partner(hop(s), -1) * 2 + c

    def src_mate(s):
        return partner(hop(s), -1) * 2 + (1 - c)

    def at(dy, dx):
        return (y + dy + ny) % ny * nx + (x + dx + nx) % nx

    def colsl(q):
        return pl.ds(pl.multiple_of(q * cols, cols), cols)

    def send(src, dst, kind, rsem, ep, tp):
        pltpu.make_async_remote_copy(
            src_ref=src, dst_ref=dst, send_sem=sent.at[kind], recv_sem=rsem,
            device_id=(ep, tp), device_id_type=MESH,
        ).start()

    def landed(view, sem):
        pltpu.make_async_copy(view, view, sem).wait()

    steps_x = range(1, nx)
    steps_y = range(1, ny)
    near = nx + ny - 2
    far = (nx - 1) * (ny - 1)

    barrier = pltpu.get_barrier_semaphore()
    for d in range(1, n_ep):
        pl.semaphore_signal(barrier, inc=1, device_id=((e + d) % n_ep, j), device_id_type=MESH)
    for t in range(1, n_tp):
        pl.semaphore_signal(barrier, inc=1, device_id=(e, (j + t) % n_tp), device_id_type=MESH)
    pl.semaphore_signal(barrier, inc=1, device_id=nxt, device_id_type=MESH)
    pl.semaphore_signal(barrier, inc=1, device_id=prv, device_id_type=MESH)

    load_x = pltpu.make_async_copy(x_h, x_own, local_sem.at[0])
    load_branch = pltpu.make_async_copy(branch_h, branch, local_sem.at[1])
    own_ow = pltpu.make_async_copy(out_w, ow.at[j], local_sem.at[2])
    load_pool = pltpu.make_async_copy(pool_h, pool_w, local_sem.at[3])
    loads = [
        pltpu.make_async_copy(gate_h.at[0], gate, local_sem.at[4]),
        pltpu.make_async_copy(up_h.at[0], up, local_sem.at[5]),
        pltpu.make_async_copy(down_h.at[0], down, local_sem.at[6]),
    ]
    write_mixer = pltpu.make_async_copy(mixer_out, mixer_h, local_sem.at[7])
    write_expert = pltpu.make_async_copy(expert_out, expert_h, local_sem.at[8])
    load_gain = pltpu.make_async_copy(ffn_gain_h, ffn_gain, local_sem.at[9])
    load_route = [
        pltpu.make_async_copy(routes_h, routes, local_sem.at[10]),
        pltpu.make_async_copy(route_w_h, route_w, local_sem.at[11]),
    ]
    load_late = [
        pltpu.make_async_copy(group_gain_h, group_gain, local_sem.at[12]),
        pltpu.make_async_copy(out_gain_h, out_gain, local_sem.at[13]),
    ]
    for load in [load_x, load_gain] + load_route + [own_ow, load_branch] + loads + [load_pool] + load_late:
        load.start()

    chunk = 16

    def norm_rows(i, _):
        r = pl.ds(pl.multiple_of(i * chunk, chunk), chunk)
        xg[e, r, :] = rms_scale(x_own[r, :].astype(f32), ffn_gain[...]).astype(bf16)
        return 0

    def norm_part():
        for load in load_route:
            load.wait()
        experts = lax.broadcasted_iota(jnp.int32, (n_ep, rows), 0)
        named = jnp.zeros((n_ep, rows), f32)
        for k in range(routes.shape[0]):
            named = named + jnp.where(routes[pl.ds(k, 1), :] == experts, route_w[pl.ds(k, 1), :], 0.0)
        wg[e] = named
        load_gain.wait()
        load_x.wait()
        lax.fori_loop(0, rows // chunk, norm_rows, 0)

    def barrier_wait():
        pl.semaphore_wait(barrier, n_ep - 1 + n_tp - 1 + 2)

    norm_part()
    barrier_wait()

    quart = out_w.shape[0] // 4
    ow_rows = [pl.ds(pl.multiple_of((c * 2 + k) * quart, quart), quart) for k in range(2)]
    my_half = pl.ds(pl.multiple_of(c * 2 * quart, quart), 2 * quart)

    def ow_own(k):
        mine = ow.at[j, ow_rows[k]]
        for dx in steps_x:
            send(mine, mine, S_O, r_one.at[R_OA + k], e, at(0, dx))
        mine = ow.at[j, ow_rows[1 - k]]
        for dy in steps_y:
            send(mine, mine, S_O, r_one.at[R_OA + k], e, at(dy, 0))

    def ow_relay():
        landed(ow.at[pl.ds(0, near), pl.ds(0, quart)], r_one.at[R_OA])
        for dx in steps_x:
            view = ow.at[at(0, -dx), ow_rows[0]]
            for dy in steps_y:
                send(view, view, S_O2, r_one.at[R_O2], e, at(dy, 0))
        for dy in steps_y:
            view = ow.at[at(-dy, 0), ow_rows[1]]
            for dx in steps_x:
                send(view, view, S_O2, r_one.at[R_O2], e, at(0, dx))

    def ow_to_mate():
        landed(ow.at[pl.ds(0, near), pl.ds(0, quart)], r_one.at[R_OB])
        landed(ow.at[pl.ds(0, far), pl.ds(0, 2 * quart)], r_one.at[R_O2])
        for t in range(1, n_tp):
            view = ow.at[(j + t) % n_tp, my_half]
            send(view, view, S_OP, r_one.at[R_OP], mate, j)

    def to_mate(d):
        if not (isinstance(d, int) and d == 0):
            landed(xg.at[0, :, pl.ds(0, far * cols)], r_x2.at[d])
        view = xg.at[src_ep(d)]
        send(view, view, S_P, r_p.at[d], mate, j)

    def send_block(m):
        view = xg.at[e, :, colsl(j)]
        send(view, view, S_Z, r_z.at[m], partner(m, 1) * 2 + c, j)

    def send_rest():
        pl.when(outer == 0)(lambda: send_block(nz - 1))

    def start_sends():
        load_branch.wait()
        tail = branch.at[pl.ds(branch.shape[0] - rim_rows, rim_rows)]
        send(tail, rim, S_RIM, r_one.at[R_RIM], nxt[0], nxt[1])
        for d in range(1, n_ep):
            send(wg.at[e], wg.at[e], S_W, r_one.at[R_W], (e + d) % n_ep, j)
        for m in range(1, nz - 1):
            send_block(m)
        pl.when(outer == 1)(lambda: send_block(nz - 1))
        to_mate(0)
        own_ow.wait()
        ow_own(0)
        ow_own(1)

    start_sends()

    branch_rows = branch.shape[0]

    def pool():
        load_pool.wait()
        for load in load_late:
            load.wait()
        landed(rim, r_one.at[R_RIM])
        chans = branch.shape[1] // len(pool_windows)
        first_row = (e * n_tp + j) * branch_rows
        positions = first_row + lax.broadcasted_iota(jnp.int32, (branch_rows, 1), 0)
        total = jnp.zeros((branch_rows, 1), f32)
        for g, window in enumerate(pool_windows):
            lanes = slice(g * chans, (g + 1) * chans)
            here = branch[:, lanes].astype(f32)
            edge = jnp.where(first_row == 0, 0.0, rim[:, lanes].astype(f32))
            wide = jnp.concatenate([edge, here], axis=0)
            reach = 1
            while reach < window:
                wide = wide + pltpu.roll(wide, reach, 0)
                reach *= 2
            counts = jnp.minimum(window, positions + 1).astype(f32)
            pooled = (wide[rim_rows:] / counts - here).astype(bf16)
            part = jnp.dot(pooled, pool_w[g], preferred_element_type=f32)
            proj[:, lanes] = part
            total = total + jnp.sum(part * part, axis=-1, keepdims=True)
        scale = lax.rsqrt(total / branch.shape[1] + norm_eps)
        mixed[...] = (proj[:, : branch.shape[1]] * scale * group_gain[...]).astype(bf16)

    def gather_one(d):
        view = xg.at[src_ep(d), :, colsl(j)]
        landed(view, r_z.at[hop(d)])
        for dx in steps_x:
            send(view, view, S_X1, r_x1.at[d], e, at(0, dx))
        for dy in steps_y:
            send(view, view, S_X1, r_x1.at[d], e, at(dy, 0))

    def gather_two(d):
        landed(xg.at[0, :, pl.ds(0, near * cols)], r_x1.at[d])
        for dx in steps_x:
            view = xg.at[src_ep(d), upper, colsl(at(0, -dx))]
            for dy in steps_y:
                send(view, view, S_X2, r_x2.at[d], e, at(dy, 0))
        for dy in steps_y:
            view = xg.at[src_ep(d), lower, colsl(at(-dy, 0))]
            for dx in steps_x:
                send(view, view, S_X2, r_x2.at[d], e, at(0, dx))

    diagonal = lax.broadcasted_iota(jnp.int32, (rows, rows), 0) == lax.broadcasted_iota(
        jnp.int32, (rows, rows), 1
    )

    def row_weights(block):
        line = wg[block, pl.ds(e, 1), :]
        return jnp.sum(jnp.where(diagonal, line, 0.0), axis=1, keepdims=True)

    step_f = min(512, gate.shape[1])
    parts_f = gate.shape[1] // step_f

    def hidden_part(s, n):
        span = pl.ds(n * step_f, step_f)
        both = jnp.concatenate([xg[src_ep(s)], xg[src_mate(s)]], axis=0)
        g = jnp.dot(both, gate[:, span], preferred_element_type=f32)
        u = jnp.dot(both, up[:, span], preferred_element_type=f32)
        g = jnp.minimum(g, clamp_limit)
        u = jnp.clip(u, -clamp_limit, clamp_limit)
        hid[:, span] = ((u + 1.0) * g * jax.nn.sigmoid(sigmoid_slope * g)).astype(bf16)

    step_d = min(1024, width)

    def down_part(s):
        mine = row_weights(src_ep(s))
        theirs = row_weights(src_mate(s))

        def one(q, _):
            span = pl.ds(pl.multiple_of(q * step_d, step_d), step_d)
            out = jnp.dot(hid[...], down[:, span], preferred_element_type=f32)
            psend[s, :, span] = (out[rows:] * theirs).astype(bf16)
            pown[s % 2, :, span] = out[:rows] * mine
            send(psend.at[s, :, span], precv.at[s, :, span], S_M, r_m.at[s], mate, j)
            return 0

        lax.fori_loop(0, width // step_d, one, 0)

    def scatter_one(s, h):
        if h == 0:
            landed(precv.at[s], r_m.at[s])
        top = pl.ds(2 * h * qr, qr)
        low = pl.ds((2 * h + 1) * qr, qr)

        def one(q, _):
            a = pown[s % 2, top, colsl(q)] + precv[s, top, colsl(q)].astype(f32)
            b = pown[s % 2, low, colsl(q)] + precv[s, low, colsl(q)].astype(f32)
            ts_a[s, h, q % nx, q // nx] = a.astype(bf16)
            ts_b[s, h, q // nx, q % nx] = b.astype(bf16)
            return 0

        lax.fori_loop(0, n_tp, one, 0)
        for dx in steps_x:
            dst = t1.at[s, h, pl.ds((dx - 1) * ny, ny)]
            send(ts_a.at[s, h, (x + dx) % nx], dst, S_T1, r_t1.at[s, h], e, at(0, dx))
        for dy in steps_y:
            dst = t1.at[s, h, pl.ds((nx - 1) * ny + (dy - 1) * nx, nx)]
            send(ts_b.at[s, h, (y + dy) % ny], dst, S_T1, r_t1.at[s, h], e, at(dy, 0))

    def scatter_two(s, h):
        landed(t1.at[s, h], r_t1.at[s, h])
        for k in range(ny):
            acc = ts_a[s, h, x, k].astype(f32)
            for dx in steps_x:
                acc = acc + t1[s, h, (dx - 1) * ny + k].astype(f32)
            u2[s, h, k] = acc.astype(bf16)
        for k in range(nx):
            acc = ts_b[s, h, y, k].astype(f32)
            for dy in steps_y:
                acc = acc + t1[s, h, (nx - 1) * ny + (dy - 1) * nx + k].astype(f32)
            u2[s, h, ny + k] = acc.astype(bf16)
        for dy in steps_y:
            send(u2.at[s, h, (y + dy) % ny], t2.at[s, h, dy - 1], S_T2, r_t2.at[s, h], e, at(dy, 0))
        for dx in steps_x:
            dst = t2.at[s, h, ny - 1 + dx - 1]
            send(u2.at[s, h, ny + (x + dx) % nx], dst, S_T2, r_t2.at[s, h], e, at(0, dx))

    def scatter_end(s, h):
        landed(t2.at[s, h], r_t2.at[s, h])
        a = u2[s, h, y].astype(f32)
        for dy in steps_y:
            a = a + t2[s, h, dy - 1].astype(f32)
        b = u2[s, h, ny + x].astype(f32)
        for dx in steps_x:
            b = b + t2[s, h, ny - 1 + dx - 1].astype(f32)
        top = pl.ds(2 * h * qr, qr)
        low = pl.ds((2 * h + 1) * qr, qr)
        if isinstance(s, int) and s == 0:
            facc[top] = a
            facc[low] = b
        else:
            fsend[s, top] = a.astype(bf16)
            fsend[s, low] = b.astype(bf16)
            part = pl.ds(2 * h * qr, 2 * qr)
            send(fsend.at[s, part], frecv.at[hop(s), part], S_F, r_one.at[R_F], src_ep(s), j)

    def project():
        landed(ow.at[pl.ds(0, n_tp - 1), pl.ds(0, 2 * quart)], r_one.at[R_OP])

        def one(q, total):
            part = jnp.dot(mixed[...], ow[q], preferred_element_type=f32)
            proj[:, colsl(q)] = part
            return total + jnp.sum(part * part, axis=-1, keepdims=True)

        total = lax.fori_loop(0, n_tp, one, jnp.zeros((branch_rows, 1), f32))
        scale = lax.rsqrt(total / width + norm_eps)

        def two(q, _):
            mixer_out[:, colsl(q)] = (proj[:, colsl(q)] * scale * out_gain[:, colsl(q)]).astype(bf16)
            return 0

        lax.fori_loop(0, n_tp, two, 0)
        write_mixer.start()

    def wait_block(s):
        landed(xg.at[0], r_p.at[s])

    def wait_first():
        for load in loads[:2]:
            load.wait()

    def wait_down():
        loads[2].wait()
        landed(wg.at[pl.ds(0, n_ep - 1)], r_one.at[R_W])

    G1, G2, TM, S1, S2, S3 = gather_one, gather_two, to_mate, scatter_one, scatter_two, scatter_end
    end = nz - 1
    plan = {
        0: (
            [(wait_first,)],
            [(send_rest,)],
            [(G1, 1), (wait_down,)],
            [(S1, 0, 0), (G2, 1), (G1, 2), (G1, 3), (pool,), (TM, 1)],
        ),
        1: ([], [(G2, 2), (S1, 0, 1)], [], [(G2, 3), (S2, 0, 0), (TM, 2), (S1, 1, 0), (S1, 1, 1)]),
        2: ([], [], [(TM, 3), (ow_relay,)], [(S2, 1, 0)]),
        end: (
            [],
            [(S1, end - 1, 0), (S2, end - 2, 1), (S1, end - 1, 1)],
            [],
            [
                (S2, end - 1, 0), (S3, end - 2, 0), (S3, end - 2, 1), (S1, end, 0), (S2, end - 1, 1),
                (S1, end, 1), (ow_to_mate,), (S3, end - 1, 0), (S2, end, 0), (S3, end - 1, 1), (S2, end, 1),
                (S2, 0, 1), (S3, 0, 0), (S3, end, 0), (project,), (S3, end, 1), (S3, 0, 1),
            ],
        ),
    }
    assert nz >= 4

    def middle(s, slot):
        if slot == 1:
            scatter_one(s - 1, 0)
            scatter_two(s - 2, 1)
            scatter_one(s - 1, 1)
        if slot == 2:
            to_mate(s + 1)
        if slot == 3:
            scatter_two(s - 1, 0)
            scatter_end(s - 2, 0)
            scatter_end(s - 2, 1)

    def run(s, slot):
        for i, slots in plan.items():
            if slots[slot]:
                @pl.when(s == i)
                def _():
                    for act in slots[slot]:
                        act[0](*act[1:])

        if nz > 4:
            if slot > 0:
                @pl.when((s > 2) & (s < end))
                def _():
                    middle(s, slot)

            if slot == 3:
                @pl.when((s > 1) & (s + 2 < nz))
                def _():
                    gather_one(s + 2)
                    gather_two(s + 2)

    def step(s, _):
        run(s, 0)
        wait_block(s)
        for n in range(parts_f):
            hidden_part(s, n)
            if n == 0:
                run(s, 1)
        run(s, 2)
        down_part(s)
        run(s, 3)
        return 0

    lax.fori_loop(0, nz, step, 0)

    def drain_all():
        write_mixer.wait()
        landed(fsend.at[pl.ds(1, nz - 1)], sent.at[S_Z])
        landed(xg.at[pl.ds(0, nz - 1), :, pl.ds(0, near * cols)], sent.at[S_X1])
        landed(xg.at[pl.ds(0, nz - 1), :, pl.ds(0, far * cols)], sent.at[S_X2])
        landed(psend, sent.at[S_P])
        landed(wg.at[pl.ds(0, n_ep - 1)], sent.at[S_W])
        landed(rim, sent.at[S_RIM])
        landed(ow.at[pl.ds(0, near), pl.ds(0, 2 * quart)], sent.at[S_O])
        landed(ow.at[pl.ds(0, far), pl.ds(0, 2 * quart)], sent.at[S_O2])
        landed(ow.at[pl.ds(0, n_tp - 1), pl.ds(0, 2 * quart)], sent.at[S_OP])
        landed(psend, sent.at[S_M])
        landed(t1, sent.at[S_T1])
        landed(t2, sent.at[S_T2])

    def final_sum():
        landed(frecv.at[pl.ds(1, nz - 1)], r_one.at[R_F])
        acc = facc[...]
        for d in range(1, nz):
            acc = acc + frecv[d].astype(f32)
        expert_out[...] = acc.astype(bf16)

    def finish():
        write_expert.start()
        landed(fsend.at[pl.ds(1, nz - 1)], sent.at[S_F])
        write_expert.wait()

    drain_all()
    final_sum()
    finish()


def per_device(
    n_ep, n_tp,
    branch_in, pool_weight, group_gain, out_weight, out_gain,
    ffn_input, ffn_gain, routes, route_weight, gate_weight, up_weight, down_weight,
):
    rows, width = ffn_input.shape
    nz = n_ep // 2
    ny, nx = grid_of(n_tp)
    cols = width // n_tp
    qr = rows // 4
    hidden = gate_weight.shape[2]
    branch_rows, branch_width = branch_in.shape
    hbm = pl.BlockSpec(memory_space=pltpu.HBM)
    anyspace = pl.BlockSpec(memory_space=pl.ANY)
    dma = pltpu.SemaphoreType.DMA
    k1 = (nx - 1) * ny + (ny - 1) * nx
    k2 = nx + ny - 2
    buffers = [
        ((1, branch_width), f32),
        ((1, width), f32),
        ((1, width), f32),
        (routes.shape[::-1], jnp.int32),
        (route_weight.shape[::-1], f32),
        ((branch_rows, branch_width), bf16),
        (pool_weight.shape, bf16),
        ((rows, width), bf16),
        ((width, hidden), bf16),
        ((width, hidden), bf16),
        ((hidden, width), bf16),
        ((n_ep, rows, width), bf16),
        ((n_ep, n_ep, rows), f32),
        ((rim_rows, branch_width), bf16),
        ((n_tp, branch_width, cols), bf16),
        ((2 * rows, hidden), bf16),
        ((branch_rows, branch_width), bf16),
        ((branch_rows, width), f32),
        ((branch_rows, width), bf16),
        ((rows, cols), bf16),
        ((2, rows, width), f32),
        ((nz, rows, width), bf16),
        ((nz, rows, width), bf16),
        ((nz, 2, nx, ny, qr, cols), bf16),
        ((nz, 2, ny, nx, qr, cols), bf16),
        ((nz, 2, k1, qr, cols), bf16),
        ((nz, 2, ny + nx, qr, cols), bf16),
        ((nz, 2, k2, qr, cols), bf16),
        ((nz, rows, cols), bf16),
        ((nz, rows, cols), bf16),
        ((rows, cols), f32),
    ]
    operands = (
        group_gain.reshape(1, -1), out_gain.reshape(1, -1), ffn_gain.reshape(1, -1), routes.T, route_weight.T,
        branch_in, pool_weight, out_weight, ffn_input, gate_weight, up_weight, down_weight,
    )
    held = sum(math.prod(shape) * jnp.dtype(kind).itemsize for shape, kind in buffers)
    return pl.pallas_call(
        functools.partial(kernel, n_ep, n_tp),
        out_shape=(
            jax.ShapeDtypeStruct((branch_rows, width), bf16),
            jax.ShapeDtypeStruct((rows, cols), bf16),
        ),
        in_specs=[hbm] * 12,
        out_specs=(anyspace, anyspace),
        scratch_shapes=[pltpu.VMEM(shape, kind) for shape, kind in buffers] + [
            dma((14,)), dma((13,)),
            dma((nz,)), dma((nz,)), dma((nz,)), dma((nz,)), dma((nz,)),
            dma((nz, 2)), dma((nz, 2)), dma((7,)),
        ],
        compiler_params=pltpu.CompilerParams(
            collective_id=0, has_side_effects=True, vmem_limit_bytes=min(67043328, held + (8 << 20))
        ),
    )(
        *[pltpu.with_memory_space_constraint(v, pltpu.HBM) for v in operands]
    )


def solution(mesh):
    in_specs = (
        P(("ep", "tp"), None),
        P(),
        P(),
        P(None, "tp"),
        P(),
        P("ep", None),
        P(),
        P("ep", None),
        P("ep", None),
        P("ep", None, "tp"),
        P("ep", None, "tp"),
        P("ep", "tp", None),
    )
    out_specs = (P(("ep", "tp"), None), P("ep", "tp"))
    return jax.shard_map(
        functools.partial(per_device, mesh.shape["ep"], mesh.shape["tp"]),
        mesh=mesh, in_specs=in_specs, out_specs=out_specs, check_vma=False,
    )
```

```python
import functools
import math
import jax
import jax.numpy as jnp
from jax import lax
from jax.experimental import pallas as pl
from jax.experimental.pallas import tpu as pltpu
from jax.sharding import PartitionSpec as P

pool_windows = (2, 4, 8, 16)
rim_rows = 16
norm_eps = 1e-06
clamp_limit = 7.0
sigmoid_slope = 1.702
MESH = pl.DeviceIdType.MESH
f32 = jnp.float32
bf16 = jnp.bfloat16


def rms_scale(values, gain):
    return values * lax.rsqrt(jnp.mean(values * values, axis=-1, keepdims=True) + norm_eps) * gain


def grid_of(n_tp):
    nx = 1
    for k in range(1, n_tp + 1):
        if n_tp % k == 0 and k * k <= n_tp:
            nx = k
    return n_tp // nx, nx


def kernel(
    n_ep, n_tp,
    group_gain_h, out_gain_h, ffn_gain_h, routes_h, route_w_h, branch_h, pool_h, out_w, x_h,
    gate_h, up_h, down_h,
    mixer_h, expert_h,
    group_gain, out_gain, ffn_gain, routes, route_w, branch, pool_w, x_own, gate, up, down, xg, wg, rim, ow, hid, mixed, proj, mixer_out, expert_out,
    pown, psend, precv, ts_a, ts_b, t1, u2, t2, fsend, frecv, facc,
    local_sem, sent, r_z, r_x1, r_x2, r_p, r_m, r_t1, r_t2, r_one,
):
    e = lax.axis_index("ep")
    j = lax.axis_index("tp")
    nz = n_ep // 2
    ny, nx = grid_of(n_tp)
    z = e // 2
    c = e % 2
    y = j // nx
    x = j % nx
    rows, width = x_own.shape
    cols = width // n_tp
    half = rows // 2
    qr = rows // 4
    upper = pl.ds(0, half)
    lower = pl.ds(half, half)
    mate = z * 2 + (1 - c)
    last = (j == n_tp - 1).astype(jnp.int32)
    first = (j == 0).astype(jnp.int32)
    nxt = ((e + last) % n_ep, (j + 1) % n_tp)
    prv = ((e - first + n_ep) % n_ep, (j - 1 + n_tp) % n_tp)
    paired = nz & (nz - 1) == 0
    S_Z, S_X1, S_X2, S_P, S_W, S_RIM, S_O, S_O2, S_OP, S_M, S_T1, S_T2, S_F, S_OZ = range(14)
    R_W, R_RIM, R_OA, R_OB, R_O2, R_OP, R_F, R_OZ = range(8)

    outer = ((z == 0) | (z == nz - 1)).astype(jnp.int32)

    def hop(s):
        if isinstance(s, int) and s == 0:
            return 0
        turned = s % (nz - 1) + 1
        return s + outer * jnp.where(s == 0, 0, turned - s)

    def partner(m, sign):
        if not paired:
            return (z + sign * m + nz) % nz
        total, bit = 0, 1
        while bit < nz:
            total = total + (z // bit + m // bit) % 2 * bit
            bit *= 2
        return total

    def src_ep(s):
        return partner(hop(s), -1) * 2 + c

    def src_mate(s):
        return partner(hop(s), -1) * 2 + (1 - c)

    def at(dy, dx):
        return (y + dy + ny) % ny * nx + (x + dx + nx) % nx

    def colsl(q):
        return pl.ds(pl.multiple_of(q * cols, cols), cols)

    def send(src, dst, kind, rsem, ep, tp):
        pltpu.make_async_remote_copy(
            src_ref=src, dst_ref=dst, send_sem=sent.at[kind], recv_sem=rsem,
            device_id=(ep, tp), device_id_type=MESH,
        ).start()

    def landed(view, sem):
        pltpu.make_async_copy(view, view, sem).wait()

    steps_x = range(1, nx)
    steps_y = range(1, ny)
    near = nx + ny - 2
    far = (nx - 1) * (ny - 1)

    barrier = pltpu.get_barrier_semaphore()
    for d in range(1, n_ep):
        pl.semaphore_signal(barrier, inc=1, device_id=((e + d) % n_ep, j), device_id_type=MESH)
    for t in range(1, n_tp):
        pl.semaphore_signal(barrier, inc=1, device_id=(e, (j + t) % n_tp), device_id_type=MESH)
    pl.semaphore_signal(barrier, inc=1, device_id=nxt, device_id_type=MESH)
    pl.semaphore_signal(barrier, inc=1, device_id=prv, device_id_type=MESH)

    load_x = pltpu.make_async_copy(x_h, x_own, local_sem.at[0])
    load_branch = pltpu.make_async_copy(branch_h, branch, local_sem.at[1])
    own_ow = pltpu.make_async_copy(out_w, ow.at[j], local_sem.at[2])
    load_pool = pltpu.make_async_copy(pool_h, pool_w, local_sem.at[3])
    loads = [
        pltpu.make_async_copy(gate_h.at[0], gate, local_sem.at[4]),
        pltpu.make_async_copy(up_h.at[0], up, local_sem.at[5]),
        pltpu.make_async_copy(down_h.at[0], down, local_sem.at[6]),
    ]
    write_mixer = pltpu.make_async_copy(mixer_out, mixer_h, local_sem.at[7])
    write_expert = pltpu.make_async_copy(expert_out, expert_h, local_sem.at[8])
    load_gain = pltpu.make_async_copy(ffn_gain_h, ffn_gain, local_sem.at[9])
    load_route = [
        pltpu.make_async_copy(routes_h, routes, local_sem.at[10]),
        pltpu.make_async_copy(route_w_h, route_w, local_sem.at[11]),
    ]
    load_late = [
        pltpu.make_async_copy(group_gain_h, group_gain, local_sem.at[12]),
        pltpu.make_async_copy(out_gain_h, out_gain, local_sem.at[13]),
    ]
    for load in [load_x, load_gain] + load_route + [own_ow, load_branch] + loads + [load_pool] + load_late:
        load.start()

    chunk = 16

    def norm_rows(i, _):
        r = pl.ds(pl.multiple_of(i * chunk, chunk), chunk)
        xg[e, r, :] = rms_scale(x_own[r, :].astype(f32), ffn_gain[...]).astype(bf16)
        return 0

    def norm_part():
        for load in load_route:
            load.wait()
        experts = lax.broadcasted_iota(jnp.int32, (n_ep, rows), 0)
        named = jnp.zeros((n_ep, rows), f32)
        for k in range(routes.shape[0]):
            named = named + jnp.where(routes[pl.ds(k, 1), :] == experts, route_w[pl.ds(k, 1), :], 0.0)
        wg[e] = named
        load_gain.wait()
        load_x.wait()
        lax.fori_loop(0, rows // chunk, norm_rows, 0)

    def barrier_wait():
        pl.semaphore_wait(barrier, n_ep - 1 + n_tp - 1 + 2)

    norm_part()
    barrier_wait()

    eighth = out_w.shape[0] // 8
    quart = 2 * eighth
    share = (c * 2 + z % 2) * quart
    ow_rows = [pl.ds(pl.multiple_of(share + k * eighth, eighth), eighth) for k in range(2)]
    my_quart = pl.ds(pl.multiple_of(share, quart), quart)
    my_half = pl.ds(pl.multiple_of(c * 2 * quart, quart), 2 * quart)

    def ow_own(k):
        mine = ow.at[j, ow_rows[k]]
        for dx in steps_x:
            send(mine, mine, S_O, r_one.at[R_OA + k], e, at(0, dx))
        mine = ow.at[j, ow_rows[1 - k]]
        for dy in steps_y:
            send(mine, mine, S_O, r_one.at[R_OA + k], e, at(dy, 0))

    def ow_relay():
        landed(ow.at[pl.ds(0, near), pl.ds(0, eighth)], r_one.at[R_OA])
        for dx in steps_x:
            view = ow.at[at(0, -dx), ow_rows[0]]
            for dy in steps_y:
                send(view, view, S_O2, r_one.at[R_O2], e, at(dy, 0))
        for dy in steps_y:
            view = ow.at[at(-dy, 0), ow_rows[1]]
            for dx in steps_x:
                send(view, view, S_O2, r_one.at[R_O2], e, at(0, dx))

    def ow_along_z():
        landed(ow.at[pl.ds(0, near), pl.ds(0, eighth)], r_one.at[R_OB])
        landed(ow.at[pl.ds(0, far), pl.ds(0, quart)], r_one.at[R_O2])
        for t in range(1, n_tp):
            view = ow.at[(j + t) % n_tp, my_quart]
            send(view, view, S_OZ, r_one.at[R_OZ], (z + 1 - z % 2 * 2) * 2 + c, j)

    def ow_to_mate():
        landed(ow.at[pl.ds(0, n_tp - 1), pl.ds(0, quart)], r_one.at[R_OZ])
        for t in range(1, n_tp):
            view = ow.at[(j + t) % n_tp, my_half]
            send(view, view, S_OP, r_one.at[R_OP], mate, j)

    def to_mate(d, rows_at, q):
        view = xg.at[src_ep(d), rows_at, colsl(q)]
        send(view, view, S_P, r_p.at[d], mate, j)

    def own_to_mate():
        send(xg.at[e], xg.at[e], S_P, r_p.at[0], mate, j)

    def send_block(m):
        view = xg.at[e, :, colsl(j)]
        send(view, view, S_Z, r_z.at[m], partner(m, 1) * 2 + c, j)

    def send_rest():
        pl.when(outer == 0)(lambda: send_block(nz - 1))

    def start_sends():
        load_branch.wait()
        tail = branch.at[pl.ds(branch.shape[0] - rim_rows, rim_rows)]
        send(tail, rim, S_RIM, r_one.at[R_RIM], nxt[0], nxt[1])
        for d in range(1, n_ep):
            send(wg.at[e], wg.at[e], S_W, r_one.at[R_W], (e + d) % n_ep, j)
        for m in range(1, nz - 1):
            send_block(m)
        pl.when(outer == 1)(lambda: send_block(nz - 1))
        own_to_mate()
        own_ow.wait()
        ow_own(0)
        ow_own(1)

    start_sends()

    branch_rows = branch.shape[0]

    def pool():
        load_pool.wait()
        for load in load_late:
            load.wait()
        landed(rim, r_one.at[R_RIM])
        chans = branch.shape[1] // len(pool_windows)
        first_row = (e * n_tp + j) * branch_rows
        positions = first_row + lax.broadcasted_iota(jnp.int32, (branch_rows, 1), 0)
        total = jnp.zeros((branch_rows, 1), f32)
        for g, window in enumerate(pool_windows):
            lanes = slice(g * chans, (g + 1) * chans)
            here = branch[:, lanes].astype(f32)
            edge = jnp.where(first_row == 0, 0.0, rim[:, lanes].astype(f32))
            wide = jnp.concatenate([edge, here], axis=0)
            reach = 1
            while reach < window:
                wide = wide + pltpu.roll(wide, reach, 0)
                reach *= 2
            counts = jnp.minimum(window, positions + 1).astype(f32)
            pooled = (wide[rim_rows:] / counts - here).astype(bf16)
            part = jnp.dot(pooled, pool_w[g], preferred_element_type=f32)
            proj[:, lanes] = part
            total = total + jnp.sum(part * part, axis=-1, keepdims=True)
        scale = lax.rsqrt(total / branch.shape[1] + norm_eps)
        mixed[...] = (proj[:, : branch.shape[1]] * scale * group_gain[...]).astype(bf16)

    def gather_one(d):
        whole = xg.at[src_ep(d), :, colsl(j)]
        landed(whole, r_z.at[hop(d)])
        parts = [xg.at[src_ep(d), r, colsl(j)] for r in (upper, lower)]
        for k in range(2):
            for dx in steps_x:
                send(parts[k], parts[k], S_X1, r_x1.at[d, k], e, at(0, dx))
            for dy in steps_y:
                send(parts[1 - k], parts[1 - k], S_X1, r_x1.at[d, k], e, at(dy, 0))
        to_mate(d, pl.ds(0, rows), j)

    def gather_two(d):
        landed(xg.at[0, upper, pl.ds(0, near * cols)], r_x1.at[d, 0])
        for dx in steps_x:
            view = xg.at[src_ep(d), upper, colsl(at(0, -dx))]
            for dy in steps_y:
                send(view, view, S_X2, r_x2.at[d], e, at(dy, 0))
        for dy in steps_y:
            view = xg.at[src_ep(d), lower, colsl(at(-dy, 0))]
            for dx in steps_x:
                send(view, view, S_X2, r_x2.at[d], e, at(0, dx))
        for dx in steps_x:
            to_mate(d, upper, at(0, -dx))
        for dy in steps_y:
            to_mate(d, lower, at(-dy, 0))

    def gather_end(d):
        landed(xg.at[0, upper, pl.ds(0, near * cols)], r_x1.at[d, 1])
        for dx in steps_x:
            to_mate(d, lower, at(0, -dx))
        for dy in steps_y:
            to_mate(d, upper, at(-dy, 0))
        landed(xg.at[0, :, pl.ds(0, far * cols)], r_x2.at[d])
        for dx in steps_x:
            for dy in steps_y:
                to_mate(d, pl.ds(0, rows), at(-dy, -dx))

    diagonal = lax.broadcasted_iota(jnp.int32, (rows, rows), 0) == lax.broadcasted_iota(
        jnp.int32, (rows, rows), 1
    )

    def row_weights(block):
        line = wg[block, pl.ds(e, 1), :]
        return jnp.sum(jnp.where(diagonal, line, 0.0), axis=1, keepdims=True)

    step_f = min(512, gate.shape[1])
    parts_f = gate.shape[1] // step_f

    def hidden_part(s, n):
        span = pl.ds(n * step_f, step_f)
        both = jnp.concatenate([xg[src_ep(s)], xg[src_mate(s)]], axis=0)
        g = jnp.dot(both, gate[:, span], preferred_element_type=f32)
        u = jnp.dot(both, up[:, span], preferred_element_type=f32)
        g = jnp.minimum(g, clamp_limit)
        u = jnp.clip(u, -clamp_limit, clamp_limit)
        hid[:, span] = ((u + 1.0) * g * jax.nn.sigmoid(sigmoid_slope * g)).astype(bf16)

    step_d = min(1024, width)

    def down_part(s):
        mine = row_weights(src_ep(s))
        theirs = row_weights(src_mate(s))

        def one(q, _):
            span = pl.ds(pl.multiple_of(q * step_d, step_d), step_d)
            out = jnp.dot(hid[...], down[:, span], preferred_element_type=f32)
            psend[s, :, span] = (out[rows:] * theirs).astype(bf16)
            pown[s % 2, :, span] = out[:rows] * mine
            send(psend.at[s, :, span], precv.at[s, :, span], S_M, r_m.at[s], mate, j)
            return 0

        lax.fori_loop(0, width // step_d, one, 0)

    def scatter_one(s, h):
        if h == 0:
            landed(precv.at[s], r_m.at[s])
        top = pl.ds(2 * h * qr, qr)
        low = pl.ds((2 * h + 1) * qr, qr)

        def one(q, _):
            a = pown[s % 2, top, colsl(q)] + precv[s, top, colsl(q)].astype(f32)
            b = pown[s % 2, low, colsl(q)] + precv[s, low, colsl(q)].astype(f32)
            ts_a[s, h, q % nx, q // nx] = a.astype(bf16)
            ts_b[s, h, q // nx, q % nx] = b.astype(bf16)
            return 0

        lax.fori_loop(0, n_tp, one, 0)
        for dx in steps_x:
            dst = t1.at[s, h, pl.ds((dx - 1) * ny, ny)]
            send(ts_a.at[s, h, (x + dx) % nx], dst, S_T1, r_t1.at[s, h], e, at(0, dx))
        for dy in steps_y:
            dst = t1.at[s, h, pl.ds((nx - 1) * ny + (dy - 1) * nx, nx)]
            send(ts_b.at[s, h, (y + dy) % ny], dst, S_T1, r_t1.at[s, h], e, at(dy, 0))

    def scatter_two(s, h):
        landed(t1.at[s, h], r_t1.at[s, h])
        for k in range(ny):
            acc = ts_a[s, h, x, k].astype(f32)
            for dx in steps_x:
                acc = acc + t1[s, h, (dx - 1) * ny + k].astype(f32)
            u2[s, h, k] = acc.astype(bf16)
        for k in range(nx):
            acc = ts_b[s, h, y, k].astype(f32)
            for dy in steps_y:
                acc = acc + t1[s, h, (nx - 1) * ny + (dy - 1) * nx + k].astype(f32)
            u2[s, h, ny + k] = acc.astype(bf16)
        for dy in steps_y:
            send(u2.at[s, h, (y + dy) % ny], t2.at[s, h, dy - 1], S_T2, r_t2.at[s, h], e, at(dy, 0))
        for dx in steps_x:
            dst = t2.at[s, h, ny - 1 + dx - 1]
            send(u2.at[s, h, ny + (x + dx) % nx], dst, S_T2, r_t2.at[s, h], e, at(0, dx))

    def scatter_end(s, h):
        landed(t2.at[s, h], r_t2.at[s, h])
        a = u2[s, h, y].astype(f32)
        for dy in steps_y:
            a = a + t2[s, h, dy - 1].astype(f32)
        b = u2[s, h, ny + x].astype(f32)
        for dx in steps_x:
            b = b + t2[s, h, ny - 1 + dx - 1].astype(f32)
        top = pl.ds(2 * h * qr, qr)
        low = pl.ds((2 * h + 1) * qr, qr)
        if isinstance(s, int) and s == 0:
            facc[top] = a
            facc[low] = b
        else:
            fsend[s, top] = a.astype(bf16)
            fsend[s, low] = b.astype(bf16)
            part = pl.ds(2 * h * qr, 2 * qr)
            send(fsend.at[s, part], frecv.at[hop(s), part], S_F, r_one.at[R_F], src_ep(s), j)

    def project():
        landed(ow.at[pl.ds(0, n_tp - 1), pl.ds(0, 2 * quart)], r_one.at[R_OP])

        def one(q, total):
            part = jnp.dot(mixed[...], ow[q], preferred_element_type=f32)
            proj[:, colsl(q)] = part
            return total + jnp.sum(part * part, axis=-1, keepdims=True)

        total = lax.fori_loop(0, n_tp, one, jnp.zeros((branch_rows, 1), f32))
        scale = lax.rsqrt(total / width + norm_eps)

        def two(q, _):
            mixer_out[:, colsl(q)] = (proj[:, colsl(q)] * scale * out_gain[:, colsl(q)]).astype(bf16)
            return 0

        lax.fori_loop(0, n_tp, two, 0)
        write_mixer.start()

    def wait_block(s):
        landed(xg.at[0], r_p.at[s])

    def wait_first():
        for load in loads[:2]:
            load.wait()

    def wait_down():
        loads[2].wait()
        landed(wg.at[pl.ds(0, n_ep - 1)], r_one.at[R_W])

    G1, G2, TM, S1, S2, S3 = gather_one, gather_two, gather_end, scatter_one, scatter_two, scatter_end
    end = nz - 1
    plan = {
        0: (
            [(wait_first,)],
            [(send_rest,), (ow_relay,)],
            [(G1, 1), (wait_down,)],
            [(G2, 1), (G1, 2), (ow_along_z,), (TM, 1), (S1, 0, 0)],
        ),
        1: (
            [],
            [(G2, 2), (G1, 3)],
            [],
            [(TM, 2), (G2, 3), (S1, 1, 0), (pool,), (S1, 1, 1), (S2, 0, 0)],
        ),
        2: ([], [], [(S1, 0, 1), (TM, 3)], [(S2, 1, 0)]),
        end: (
            [],
            [(S1, end - 1, 0)],
            [(S2, end - 2, 1), (S1, end - 1, 1)],
            [
                (S3, 0, 0), (S2, end - 1, 0), (S3, end - 2, 0), (S3, end - 2, 1), (S1, end, 0),
                (S2, end - 1, 1), (S1, end, 1), (ow_to_mate,), (S3, end - 1, 0), (S2, 0, 1), (S2, end, 0),
                (S3, end - 1, 1), (S2, end, 1), (S3, 0, 1), (S3, end, 0), (S3, end, 1), (project,),
            ],
        ),
    }
    assert nz >= 4 and nz % 2 == 0

    def middle(s, slot):
        if slot == 1:
            scatter_one(s - 1, 0)
        if slot == 2:
            scatter_two(s - 2, 1)
            scatter_one(s - 1, 1)
            gather_end(s + 1)
        if slot == 3:
            scatter_two(s - 1, 0)
            scatter_end(s - 2, 0)
            scatter_end(s - 2, 1)

    def run(s, slot):
        for i, slots in plan.items():
            if slots[slot]:
                @pl.when(s == i)
                def _():
                    for act in slots[slot]:
                        act[0](*act[1:])

        if nz > 4:
            if slot > 0:
                @pl.when((s > 2) & (s < end))
                def _():
                    middle(s, slot)

            if slot == 3:
                @pl.when((s > 1) & (s + 2 < nz))
                def _():
                    gather_one(s + 2)
                    gather_two(s + 2)

    def step(s, _):
        run(s, 0)
        wait_block(s)
        for n in range(parts_f):
            hidden_part(s, n)
            if n == 0:
                run(s, 1)
        run(s, 2)
        down_part(s)
        run(s, 3)
        return 0

    lax.fori_loop(0, nz, step, 0)

    def drain_all():
        landed(fsend.at[pl.ds(1, nz - 1)], sent.at[S_Z])
        landed(xg.at[pl.ds(0, nz - 1), :, pl.ds(0, near * cols)], sent.at[S_X1])
        landed(xg.at[pl.ds(0, nz - 1), :, pl.ds(0, far * cols)], sent.at[S_X2])
        landed(psend, sent.at[S_P])
        landed(wg.at[pl.ds(0, n_ep - 1)], sent.at[S_W])
        landed(rim, sent.at[S_RIM])
        landed(ow.at[pl.ds(0, near), pl.ds(0, quart)], sent.at[S_O])
        landed(ow.at[pl.ds(0, far), pl.ds(0, quart)], sent.at[S_O2])
        landed(ow.at[pl.ds(0, n_tp - 1), pl.ds(0, quart)], sent.at[S_OZ])
        landed(ow.at[pl.ds(0, n_tp - 1), pl.ds(0, 2 * quart)], sent.at[S_OP])
        landed(psend, sent.at[S_M])
        landed(t1, sent.at[S_T1])
        landed(t2, sent.at[S_T2])

    def final_sum():
        landed(frecv.at[pl.ds(1, nz - 1)], r_one.at[R_F])
        acc = facc[...]
        for d in range(1, nz):
            acc = acc + frecv[d].astype(f32)
        expert_out[...] = acc.astype(bf16)

    def finish():
        write_expert.start()
        write_mixer.wait()
        landed(fsend.at[pl.ds(1, nz - 1)], sent.at[S_F])
        write_expert.wait()

    drain_all()
    final_sum()
    finish()


def per_device(
    n_ep, n_tp,
    branch_in, pool_weight, group_gain, out_weight, out_gain,
    ffn_input, ffn_gain, routes, route_weight, gate_weight, up_weight, down_weight,
):
    rows, width = ffn_input.shape
    nz = n_ep // 2
    ny, nx = grid_of(n_tp)
    cols = width // n_tp
    qr = rows // 4
    hidden = gate_weight.shape[2]
    branch_rows, branch_width = branch_in.shape
    hbm = pl.BlockSpec(memory_space=pltpu.HBM)
    anyspace = pl.BlockSpec(memory_space=pl.ANY)
    dma = pltpu.SemaphoreType.DMA
    k1 = (nx - 1) * ny + (ny - 1) * nx
    k2 = nx + ny - 2
    buffers = [
        ((1, branch_width), f32),
        ((1, width), f32),
        ((1, width), f32),
        (routes.shape[::-1], jnp.int32),
        (route_weight.shape[::-1], f32),
        ((branch_rows, branch_width), bf16),
        (pool_weight.shape, bf16),
        ((rows, width), bf16),
        ((width, hidden), bf16),
        ((width, hidden), bf16),
        ((hidden, width), bf16),
        ((n_ep, rows, width), bf16),
        ((n_ep, n_ep, rows), f32),
        ((rim_rows, branch_width), bf16),
        ((n_tp, branch_width, cols), bf16),
        ((2 * rows, hidden), bf16),
        ((branch_rows, branch_width), bf16),
        ((branch_rows, width), f32),
        ((branch_rows, width), bf16),
        ((rows, cols), bf16),
        ((2, rows, width), f32),
        ((nz, rows, width), bf16),
        ((nz, rows, width), bf16),
        ((nz, 2, nx, ny, qr, cols), bf16),
        ((nz, 2, ny, nx, qr, cols), bf16),
        ((nz, 2, k1, qr, cols), bf16),
        ((nz, 2, ny + nx, qr, cols), bf16),
        ((nz, 2, k2, qr, cols), bf16),
        ((nz, rows, cols), bf16),
        ((nz, rows, cols), bf16),
        ((rows, cols), f32),
    ]
    operands = (
        group_gain.reshape(1, -1), out_gain.reshape(1, -1), ffn_gain.reshape(1, -1), routes.T, route_weight.T,
        branch_in, pool_weight, out_weight, ffn_input, gate_weight, up_weight, down_weight,
    )
    held = sum(math.prod(shape) * jnp.dtype(kind).itemsize for shape, kind in buffers)
    return pl.pallas_call(
        functools.partial(kernel, n_ep, n_tp),
        out_shape=(
            jax.ShapeDtypeStruct((branch_rows, width), bf16),
            jax.ShapeDtypeStruct((rows, cols), bf16),
        ),
        in_specs=[hbm] * 12,
        out_specs=(anyspace, anyspace),
        scratch_shapes=[pltpu.VMEM(shape, kind) for shape, kind in buffers] + [
            dma((14,)), dma((14,)),
            dma((nz,)), dma((nz, 2)), dma((nz,)), dma((nz,)), dma((nz,)),
            dma((nz, 2)), dma((nz, 2)), dma((8,)),
        ],
        compiler_params=pltpu.CompilerParams(
            collective_id=0, has_side_effects=True, vmem_limit_bytes=min(67043328, held + (8 << 20))
        ),
    )(
        *[pltpu.with_memory_space_constraint(v, pltpu.HBM) for v in operands]
    )


def solution(mesh):
    in_specs = (
        P(("ep", "tp"), None),
        P(),
        P(),
        P(None, "tp"),
        P(),
        P("ep", None),
        P(),
        P("ep", None),
        P("ep", None),
        P("ep", None, "tp"),
        P("ep", None, "tp"),
        P("ep", "tp", None),
    )
    out_specs = (P(("ep", "tp"), None), P("ep", "tp"))
    return jax.shard_map(
        functools.partial(per_device, mesh.shape["ep"], mesh.shape["tp"]),
        mesh=mesh, in_specs=in_specs, out_specs=out_specs, check_vma=False,
    )
```

```python
import functools
import math
import jax
import jax.numpy as jnp
from jax import lax
from jax.experimental import pallas as pl
from jax.experimental.pallas import tpu as pltpu
from jax.sharding import PartitionSpec as P

pool_windows = (2, 4, 8, 16)
rim_rows = 16
norm_eps = 1e-06
clamp_limit = 7.0
sigmoid_slope = 1.702
MESH = pl.DeviceIdType.MESH
f32 = jnp.float32
bf16 = jnp.bfloat16


def rms_scale(values, gain):
    return values * lax.rsqrt(jnp.mean(values * values, axis=-1, keepdims=True) + norm_eps) * gain


def grid_of(n_tp):
    nx = 1
    for k in range(1, n_tp + 1):
        if n_tp % k == 0 and k * k <= n_tp:
            nx = k
    return n_tp // nx, nx


def kernel(
    n_ep, n_tp,
    group_gain_h, out_gain_h, ffn_gain_h, routes_h, route_w_h, branch_h, pool_h, out_w, x_h,
    gate_h, up_h, down_h,
    mixer_h, expert_h,
    group_gain, out_gain, ffn_gain, routes, route_w, branch, pool_w, x_own, gate, up, down, xg, wg, rim, ow, hid, mixed, proj, mixer_out, expert_out,
    pown, psend, precv, ts_a, ts_b, t1, u2, t2, fsend, frecv, facc,
    local_sem, sent, r_z, r_x1, r_x2, r_p, r_m, r_t1, r_t2, r_one,
):
    e = lax.axis_index("ep")
    j = lax.axis_index("tp")
    nz = n_ep // 2
    ny, nx = grid_of(n_tp)
    z = e // 2
    c = e % 2
    y = j // nx
    x = j % nx
    rows, width = x_own.shape
    cols = width // n_tp
    half = rows // 2
    qr = rows // 4
    upper = pl.ds(0, half)
    lower = pl.ds(half, half)
    mate = z * 2 + (1 - c)
    last = (j == n_tp - 1).astype(jnp.int32)
    first = (j == 0).astype(jnp.int32)
    nxt = ((e + last) % n_ep, (j + 1) % n_tp)
    prv = ((e - first + n_ep) % n_ep, (j - 1 + n_tp) % n_tp)
    paired = nz & (nz - 1) == 0
    S_Z, S_X1, S_X2, S_P, S_W, S_RIM, S_O, S_O2, S_OP, S_M, S_T1, S_T2, S_F, S_OZ = range(14)
    R_W, R_RIM, R_OA, R_OB, R_O2, R_OP, R_F, R_OZ = range(8)

    outer = ((z == 0) | (z == nz - 1)).astype(jnp.int32)

    def hop(s):
        if isinstance(s, int) and s == 0:
            return 0
        turned = s % (nz - 1) + 1
        return s + outer * jnp.where(s == 0, 0, turned - s)

    def partner(m, sign):
        if not paired:
            return (z + sign * m + nz) % nz
        total, bit = 0, 1
        while bit < nz:
            total = total + (z // bit + m // bit) % 2 * bit
            bit *= 2
        return total

    def src_ep(s):
        return partner(hop(s), -1) * 2 + c

    def src_mate(s):
        return partner(hop(s), -1) * 2 + (1 - c)

    def at(dy, dx):
        return (y + dy + ny) % ny * nx + (x + dx + nx) % nx

    def colsl(q):
        return pl.ds(pl.multiple_of(q * cols, cols), cols)

    def send(src, dst, kind, rsem, ep, tp):
        pltpu.make_async_remote_copy(
            src_ref=src, dst_ref=dst, send_sem=sent.at[kind], recv_sem=rsem,
            device_id=(ep, tp), device_id_type=MESH,
        ).start()

    def landed(view, sem):
        pltpu.make_async_copy(view, view, sem).wait()

    steps_x = range(1, nx)
    steps_y = range(1, ny)
    near = nx + ny - 2
    far = (nx - 1) * (ny - 1)

    barrier = pltpu.get_barrier_semaphore()
    for d in range(1, n_ep):
        pl.semaphore_signal(barrier, inc=1, device_id=((e + d) % n_ep, j), device_id_type=MESH)
    for t in range(1, n_tp):
        pl.semaphore_signal(barrier, inc=1, device_id=(e, (j + t) % n_tp), device_id_type=MESH)
    pl.semaphore_signal(barrier, inc=1, device_id=nxt, device_id_type=MESH)
    pl.semaphore_signal(barrier, inc=1, device_id=prv, device_id_type=MESH)

    load_x = pltpu.make_async_copy(x_h, x_own, local_sem.at[0])
    load_branch = pltpu.make_async_copy(branch_h, branch, local_sem.at[1])
    own_ow = pltpu.make_async_copy(out_w, ow.at[j], local_sem.at[2])
    load_pool = pltpu.make_async_copy(pool_h, pool_w, local_sem.at[3])
    loads = [
        pltpu.make_async_copy(gate_h.at[0], gate, local_sem.at[4]),
        pltpu.make_async_copy(up_h.at[0], up, local_sem.at[5]),
        pltpu.make_async_copy(down_h.at[0], down, local_sem.at[6]),
    ]
    write_mixer = pltpu.make_async_copy(mixer_out, mixer_h, local_sem.at[7])
    write_expert = pltpu.make_async_copy(expert_out, expert_h, local_sem.at[8])
    load_gain = pltpu.make_async_copy(ffn_gain_h, ffn_gain, local_sem.at[9])
    load_route = [
        pltpu.make_async_copy(routes_h, routes, local_sem.at[10]),
        pltpu.make_async_copy(route_w_h, route_w, local_sem.at[11]),
    ]
    load_late = [
        pltpu.make_async_copy(group_gain_h, group_gain, local_sem.at[12]),
        pltpu.make_async_copy(out_gain_h, out_gain, local_sem.at[13]),
    ]
    for load in [load_x, load_gain] + load_route + [own_ow, load_branch] + loads + [load_pool] + load_late:
        load.start()

    chunk = 16

    def norm_rows(i, _):
        r = pl.ds(pl.multiple_of(i * chunk, chunk), chunk)
        xg[e, r, :] = rms_scale(x_own[r, :].astype(f32), ffn_gain[...]).astype(bf16)
        return 0

    def norm_part():
        for load in load_route:
            load.wait()
        experts = lax.broadcasted_iota(jnp.int32, (n_ep, rows), 0)
        named = jnp.zeros((n_ep, rows), f32)
        for k in range(routes.shape[0]):
            named = named + jnp.where(routes[pl.ds(k, 1), :] == experts, route_w[pl.ds(k, 1), :], 0.0)
        wg[e] = named
        load_gain.wait()
        load_x.wait()
        lax.fori_loop(0, rows // chunk, norm_rows, 0)

    def barrier_wait():
        pl.semaphore_wait(barrier, n_ep - 1 + n_tp - 1 + 2)

    norm_part()
    barrier_wait()

    eighth = out_w.shape[0] // 8
    quart = 2 * eighth
    share = (c * 2 + z % 2) * quart
    ow_rows = [pl.ds(pl.multiple_of(share + k * eighth, eighth), eighth) for k in range(2)]
    my_quart = pl.ds(pl.multiple_of(share, quart), quart)
    my_half = pl.ds(pl.multiple_of(c * 2 * quart, quart), 2 * quart)

    def ow_own(k):
        mine = ow.at[j, ow_rows[k]]
        for dx in steps_x:
            send(mine, mine, S_O, r_one.at[R_OA + k], e, at(0, dx))
        mine = ow.at[j, ow_rows[1 - k]]
        for dy in steps_y:
            send(mine, mine, S_O, r_one.at[R_OA + k], e, at(dy, 0))

    def ow_relay():
        landed(ow.at[pl.ds(0, near), pl.ds(0, eighth)], r_one.at[R_OA])
        for dx in steps_x:
            view = ow.at[at(0, -dx), ow_rows[0]]
            for dy in steps_y:
                send(view, view, S_O2, r_one.at[R_O2], e, at(dy, 0))
        for dy in steps_y:
            view = ow.at[at(-dy, 0), ow_rows[1]]
            for dx in steps_x:
                send(view, view, S_O2, r_one.at[R_O2], e, at(0, dx))

    def ow_along_z():
        landed(ow.at[pl.ds(0, near), pl.ds(0, eighth)], r_one.at[R_OB])
        landed(ow.at[pl.ds(0, far), pl.ds(0, quart)], r_one.at[R_O2])
        for t in range(1, n_tp):
            view = ow.at[(j + t) % n_tp, my_quart]
            send(view, view, S_OZ, r_one.at[R_OZ], (z + 1 - z % 2 * 2) * 2 + c, j)

    def ow_to_mate():
        landed(ow.at[pl.ds(0, n_tp - 1), pl.ds(0, quart)], r_one.at[R_OZ])
        for t in range(1, n_tp):
            view = ow.at[(j + t) % n_tp, my_half]
            send(view, view, S_OP, r_one.at[R_OP], mate, j)

    def to_mate(d, rows_at, q):
        view = xg.at[src_ep(d), rows_at, colsl(q)]
        send(view, view, S_P, r_p.at[d], mate, j)

    def own_to_mate():
        send(xg.at[e], xg.at[e], S_P, r_p.at[0], mate, j)

    def send_block(m):
        view = xg.at[e, :, colsl(j)]
        send(view, view, S_Z, r_z.at[m], partner(m, 1) * 2 + c, j)

    def send_rest():
        pl.when(outer == 0)(lambda: send_block(nz - 1))

    def start_sends():
        load_branch.wait()
        tail = branch.at[pl.ds(branch.shape[0] - rim_rows, rim_rows)]
        send(tail, rim, S_RIM, r_one.at[R_RIM], nxt[0], nxt[1])
        for d in range(1, n_ep):
            send(wg.at[e], wg.at[e], S_W, r_one.at[R_W], (e + d) % n_ep, j)
        for m in range(1, nz - 1):
            send_block(m)
        pl.when(outer == 1)(lambda: send_block(nz - 1))
        own_to_mate()
        own_ow.wait()
        ow_own(0)
        ow_own(1)

    start_sends()

    branch_rows = branch.shape[0]

    def pool():
        load_pool.wait()
        for load in load_late:
            load.wait()
        landed(rim, r_one.at[R_RIM])
        chans = branch.shape[1] // len(pool_windows)
        first_row = (e * n_tp + j) * branch_rows
        positions = first_row + lax.broadcasted_iota(jnp.int32, (branch_rows, 1), 0)
        total = jnp.zeros((branch_rows, 1), f32)
        for g, window in enumerate(pool_windows):
            lanes = slice(g * chans, (g + 1) * chans)
            here = branch[:, lanes].astype(f32)
            edge = jnp.where(first_row == 0, 0.0, rim[:, lanes].astype(f32))
            wide = jnp.concatenate([edge, here], axis=0)
            reach = 1
            while reach < window:
                wide = wide + pltpu.roll(wide, reach, 0)
                reach *= 2
            counts = jnp.minimum(window, positions + 1).astype(f32)
            pooled = (wide[rim_rows:] / counts - here).astype(bf16)
            part = jnp.dot(pooled, pool_w[g], preferred_element_type=f32)
            proj[:, lanes] = part
            total = total + jnp.sum(part * part, axis=-1, keepdims=True)
        scale = lax.rsqrt(total / branch.shape[1] + norm_eps)
        mixed[...] = (proj[:, : branch.shape[1]] * scale * group_gain[...]).astype(bf16)

    def gather_one(d):
        whole = xg.at[src_ep(d), :, colsl(j)]
        landed(whole, r_z.at[hop(d)])
        parts = [xg.at[src_ep(d), r, colsl(j)] for r in (upper, lower)]
        for k in range(2):
            for dx in steps_x:
                send(parts[k], parts[k], S_X1, r_x1.at[d, k], e, at(0, dx))
            for dy in steps_y:
                send(parts[1 - k], parts[1 - k], S_X1, r_x1.at[d, k], e, at(dy, 0))
        to_mate(d, pl.ds(0, rows), j)

    def gather_two(d):
        landed(xg.at[0, upper, pl.ds(0, near * cols)], r_x1.at[d, 0])
        for dx in steps_x:
            view = xg.at[src_ep(d), upper, colsl(at(0, -dx))]
            for dy in steps_y:
                send(view, view, S_X2, r_x2.at[d], e, at(dy, 0))
        for dy in steps_y:
            view = xg.at[src_ep(d), lower, colsl(at(-dy, 0))]
            for dx in steps_x:
                send(view, view, S_X2, r_x2.at[d], e, at(0, dx))
        for dx in steps_x:
            to_mate(d, upper, at(0, -dx))
        for dy in steps_y:
            to_mate(d, lower, at(-dy, 0))

    def gather_end(d):
        landed(xg.at[0, upper, pl.ds(0, near * cols)], r_x1.at[d, 1])
        for dx in steps_x:
            to_mate(d, lower, at(0, -dx))
        for dy in steps_y:
            to_mate(d, upper, at(-dy, 0))
        landed(xg.at[0, :, pl.ds(0, far * cols)], r_x2.at[d])
        for dx in steps_x:
            for dy in steps_y:
                to_mate(d, pl.ds(0, rows), at(-dy, -dx))

    diagonal = lax.broadcasted_iota(jnp.int32, (rows, rows), 0) == lax.broadcasted_iota(
        jnp.int32, (rows, rows), 1
    )

    def row_weights(block):
        line = wg[block, pl.ds(e, 1), :]
        return jnp.sum(jnp.where(diagonal, line, 0.0), axis=1, keepdims=True)

    step_f = min(512, gate.shape[1])
    parts_f = gate.shape[1] // step_f

    def hidden_part(s, n):
        span = pl.ds(n * step_f, step_f)
        both = jnp.concatenate([xg[src_ep(s)], xg[src_mate(s)]], axis=0)
        g = jnp.dot(both, gate[:, span], preferred_element_type=f32)
        u = jnp.dot(both, up[:, span], preferred_element_type=f32)
        g = jnp.minimum(g, clamp_limit)
        u = jnp.clip(u, -clamp_limit, clamp_limit)
        hid[:, span] = ((u + 1.0) * g * jax.nn.sigmoid(sigmoid_slope * g)).astype(bf16)

    def down_part(s):
        theirs = row_weights(src_mate(s))
        mine = row_weights(src_ep(s))
        out = jnp.dot(hid[rows:], down[...], preferred_element_type=f32)
        psend[s] = (out * theirs).astype(bf16)
        send(psend.at[s], precv.at[s], S_M, r_m.at[s], mate, j)
        out = jnp.dot(hid[:rows], down[...], preferred_element_type=f32)
        pown[s % 2] = out * mine

    def scatter_one(s, h):
        if h == 0:
            landed(precv.at[s], r_m.at[s])
        top = pl.ds(2 * h * qr, qr)
        low = pl.ds((2 * h + 1) * qr, qr)

        def one(q, _):
            a = pown[s % 2, top, colsl(q)] + precv[s, top, colsl(q)].astype(f32)
            b = pown[s % 2, low, colsl(q)] + precv[s, low, colsl(q)].astype(f32)
            ts_a[s, h, q % nx, q // nx] = a.astype(bf16)
            ts_b[s, h, q // nx, q % nx] = b.astype(bf16)
            return 0

        lax.fori_loop(0, n_tp, one, 0)
        for dx in steps_x:
            dst = t1.at[s, h, pl.ds((dx - 1) * ny, ny)]
            send(ts_a.at[s, h, (x + dx) % nx], dst, S_T1, r_t1.at[s, h], e, at(0, dx))
        for dy in steps_y:
            dst = t1.at[s, h, pl.ds((nx - 1) * ny + (dy - 1) * nx, nx)]
            send(ts_b.at[s, h, (y + dy) % ny], dst, S_T1, r_t1.at[s, h], e, at(dy, 0))

    def scatter_two(s, h):
        landed(t1.at[s, h], r_t1.at[s, h])
        for k in range(ny):
            acc = ts_a[s, h, x, k].astype(f32)
            for dx in steps_x:
                acc = acc + t1[s, h, (dx - 1) * ny + k].astype(f32)
            u2[s, h, k] = acc.astype(bf16)
        for k in range(nx):
            acc = ts_b[s, h, y, k].astype(f32)
            for dy in steps_y:
                acc = acc + t1[s, h, (nx - 1) * ny + (dy - 1) * nx + k].astype(f32)
            u2[s, h, ny + k] = acc.astype(bf16)
        for dy in steps_y:
            send(u2.at[s, h, (y + dy) % ny], t2.at[s, h, dy - 1], S_T2, r_t2.at[s, h], e, at(dy, 0))
        for dx in steps_x:
            dst = t2.at[s, h, ny - 1 + dx - 1]
            send(u2.at[s, h, ny + (x + dx) % nx], dst, S_T2, r_t2.at[s, h], e, at(0, dx))

    def scatter_end(s, h):
        landed(t2.at[s, h], r_t2.at[s, h])
        a = u2[s, h, y].astype(f32)
        for dy in steps_y:
            a = a + t2[s, h, dy - 1].astype(f32)
        b = u2[s, h, ny + x].astype(f32)
        for dx in steps_x:
            b = b + t2[s, h, ny - 1 + dx - 1].astype(f32)
        top = pl.ds(2 * h * qr, qr)
        low = pl.ds((2 * h + 1) * qr, qr)
        if isinstance(s, int) and s == 0:
            facc[top] = a
            facc[low] = b
        else:
            fsend[s, top] = a.astype(bf16)
            fsend[s, low] = b.astype(bf16)
            part = pl.ds(2 * h * qr, 2 * qr)
            send(fsend.at[s, part], frecv.at[hop(s), part], S_F, r_one.at[R_F], src_ep(s), j)

    def project():
        landed(ow.at[pl.ds(0, n_tp - 1), pl.ds(0, 2 * quart)], r_one.at[R_OP])

        def one(q, total):
            part = jnp.dot(mixed[...], ow[q], preferred_element_type=f32)
            proj[:, colsl(q)] = part
            return total + jnp.sum(part * part, axis=-1, keepdims=True)

        total = lax.fori_loop(0, n_tp, one, jnp.zeros((branch_rows, 1), f32))
        scale = lax.rsqrt(total / width + norm_eps)

        def two(q, _):
            mixer_out[:, colsl(q)] = (proj[:, colsl(q)] * scale * out_gain[:, colsl(q)]).astype(bf16)
            return 0

        lax.fori_loop(0, n_tp, two, 0)
        write_mixer.start()

    def wait_block(s):
        landed(xg.at[0], r_p.at[s])

    def wait_first():
        for load in loads[:2]:
            load.wait()

    def wait_down():
        loads[2].wait()
        landed(wg.at[pl.ds(0, n_ep - 1)], r_one.at[R_W])

    G1, G2, TM, S1, S2, S3 = gather_one, gather_two, gather_end, scatter_one, scatter_two, scatter_end
    end = nz - 1
    plan = {
        0: (
            [(wait_first,)],
            [(ow_relay,)],
            [(G1, 1), (wait_down,)],
            [(send_rest,), (G2, 1), (G1, 2), (ow_along_z,), (pool,), (TM, 1), (S1, 0, 0)],
        ),
        1: (
            [],
            [(G2, 2), (G1, 3)],
            [],
            [(TM, 2), (G2, 3), (S1, 1, 0), (S1, 1, 1), (S2, 0, 0)],
        ),
        2: ([], [], [(S1, 0, 1), (TM, 3)], [(S2, 1, 0)]),
        end: (
            [],
            [(S1, end - 1, 0)],
            [(S2, end - 2, 1), (S1, end - 1, 1)],
            [
                (S3, 0, 0), (S2, end - 1, 0), (S3, end - 2, 0), (S3, end - 2, 1), (S1, end, 0),
                (S1, end, 1), (S2, end - 1, 1), (ow_to_mate,), (S3, end - 1, 0), (S2, 0, 1), (S2, end, 0),
                (S3, end - 1, 1), (S2, end, 1), (S3, 0, 1), (S3, end, 0), (S3, end, 1), (project,),
            ],
        ),
    }
    assert nz >= 4 and nz % 2 == 0

    def middle(s, slot):
        if slot == 1:
            scatter_one(s - 1, 0)
        if slot == 2:
            scatter_two(s - 2, 1)
            scatter_one(s - 1, 1)
            gather_end(s + 1)
        if slot == 3:
            scatter_two(s - 1, 0)
            scatter_end(s - 2, 0)
            scatter_end(s - 2, 1)

    def run(s, slot):
        for i, slots in plan.items():
            if slots[slot]:
                @pl.when(s == i)
                def _():
                    for act in slots[slot]:
                        act[0](*act[1:])

        if nz > 4:
            if slot > 0:
                @pl.when((s > 2) & (s < end))
                def _():
                    middle(s, slot)

            if slot == 3:
                @pl.when((s > 1) & (s + 2 < nz))
                def _():
                    gather_one(s + 2)
                    gather_two(s + 2)

    def step(s, _):
        run(s, 0)
        wait_block(s)
        for n in range(parts_f):
            hidden_part(s, n)
            if n == 0:
                run(s, 1)
        run(s, 2)
        down_part(s)
        run(s, 3)
        return 0

    lax.fori_loop(0, nz, step, 0)

    def drain_all():
        landed(fsend.at[pl.ds(1, nz - 1)], sent.at[S_Z])
        landed(xg.at[pl.ds(0, nz - 1), :, pl.ds(0, near * cols)], sent.at[S_X1])
        landed(xg.at[pl.ds(0, nz - 1), :, pl.ds(0, far * cols)], sent.at[S_X2])
        landed(psend, sent.at[S_P])
        landed(wg.at[pl.ds(0, n_ep - 1)], sent.at[S_W])
        landed(rim, sent.at[S_RIM])
        landed(ow.at[pl.ds(0, near), pl.ds(0, quart)], sent.at[S_O])
        landed(ow.at[pl.ds(0, far), pl.ds(0, quart)], sent.at[S_O2])
        landed(ow.at[pl.ds(0, n_tp - 1), pl.ds(0, quart)], sent.at[S_OZ])
        landed(ow.at[pl.ds(0, n_tp - 1), pl.ds(0, 2 * quart)], sent.at[S_OP])
        landed(psend, sent.at[S_M])
        landed(t1, sent.at[S_T1])
        landed(t2, sent.at[S_T2])

    def final_sum():
        landed(frecv.at[pl.ds(1, nz - 1)], r_one.at[R_F])
        acc = facc[...]
        for d in range(1, nz):
            acc = acc + frecv[d].astype(f32)
        expert_out[...] = acc.astype(bf16)

    def finish():
        write_expert.start()
        write_mixer.wait()
        landed(fsend.at[pl.ds(1, nz - 1)], sent.at[S_F])
        write_expert.wait()

    drain_all()
    final_sum()
    finish()


def per_device(
    n_ep, n_tp,
    branch_in, pool_weight, group_gain, out_weight, out_gain,
    ffn_input, ffn_gain, routes, route_weight, gate_weight, up_weight, down_weight,
):
    rows, width = ffn_input.shape
    nz = n_ep // 2
    ny, nx = grid_of(n_tp)
    cols = width // n_tp
    qr = rows // 4
    hidden = gate_weight.shape[2]
    branch_rows, branch_width = branch_in.shape
    hbm = pl.BlockSpec(memory_space=pltpu.HBM)
    anyspace = pl.BlockSpec(memory_space=pl.ANY)
    dma = pltpu.SemaphoreType.DMA
    k1 = (nx - 1) * ny + (ny - 1) * nx
    k2 = nx + ny - 2
    buffers = [
        ((1, branch_width), f32),
        ((1, width), f32),
        ((1, width), f32),
        (routes.shape[::-1], jnp.int32),
        (route_weight.shape[::-1], f32),
        ((branch_rows, branch_width), bf16),
        (pool_weight.shape, bf16),
        ((rows, width), bf16),
        ((width, hidden), bf16),
        ((width, hidden), bf16),
        ((hidden, width), bf16),
        ((n_ep, rows, width), bf16),
        ((n_ep, n_ep, rows), f32),
        ((rim_rows, branch_width), bf16),
        ((n_tp, branch_width, cols), bf16),
        ((2 * rows, hidden), bf16),
        ((branch_rows, branch_width), bf16),
        ((branch_rows, width), f32),
        ((branch_rows, width), bf16),
        ((rows, cols), bf16),
        ((2, rows, width), f32),
        ((nz, rows, width), bf16),
        ((nz, rows, width), bf16),
        ((nz, 2, nx, ny, qr, cols), bf16),
        ((nz, 2, ny, nx, qr, cols), bf16),
        ((nz, 2, k1, qr, cols), bf16),
        ((nz, 2, ny + nx, qr, cols), bf16),
        ((nz, 2, k2, qr, cols), bf16),
        ((nz, rows, cols), bf16),
        ((nz, rows, cols), bf16),
        ((rows, cols), f32),
    ]
    operands = (
        group_gain.reshape(1, -1), out_gain.reshape(1, -1), ffn_gain.reshape(1, -1), routes.T, route_weight.T,
        branch_in, pool_weight, out_weight, ffn_input, gate_weight, up_weight, down_weight,
    )
    held = sum(math.prod(shape) * jnp.dtype(kind).itemsize for shape, kind in buffers)
    return pl.pallas_call(
        functools.partial(kernel, n_ep, n_tp),
        out_shape=(
            jax.ShapeDtypeStruct((branch_rows, width), bf16),
            jax.ShapeDtypeStruct((rows, cols), bf16),
        ),
        in_specs=[hbm] * 12,
        out_specs=(anyspace, anyspace),
        scratch_shapes=[pltpu.VMEM(shape, kind) for shape, kind in buffers] + [
            dma((14,)), dma((14,)),
            dma((nz,)), dma((nz, 2)), dma((nz,)), dma((nz,)), dma((nz,)),
            dma((nz, 2)), dma((nz, 2)), dma((8,)),
        ],
        compiler_params=pltpu.CompilerParams(
            collective_id=0, has_side_effects=True, vmem_limit_bytes=min(67043328, held + (8 << 20))
        ),
    )(
        *[pltpu.with_memory_space_constraint(v, pltpu.HBM) for v in operands]
    )


def solution(mesh):
    in_specs = (
        P(("ep", "tp"), None),
        P(),
        P(),
        P(None, "tp"),
        P(),
        P("ep", None),
        P(),
        P("ep", None),
        P("ep", None),
        P("ep", None, "tp"),
        P("ep", None, "tp"),
        P("ep", "tp", None),
    )
    out_specs = (P(("ep", "tp"), None), P("ep", "tp"))
    return jax.shard_map(
        functools.partial(per_device, mesh.shape["ep"], mesh.shape["tp"]),
        mesh=mesh, in_specs=in_specs, out_specs=out_specs, check_vma=False,
    )
```
